32 devices in a mesh: sp: 8 (over z, y), tp: 4 (over x, core).
Axes of the slice: x: 2, y: 2, z: 4, core: 2. Of those that a mesh axis runs over, the one named last changes fastest.
Arguments:
- tokens: bfloat16 [6144, 2048], P('sp', 'tp'), may hold values from -6 to 6
- norm_gain: float32 [2048], replicated, may hold values from 0.1 to 1.9
- w_query: bfloat16 [2048, 2048], P(None, 'tp'), may hold values from -4 to 4
- w_key: bfloat16 [2048, 2048], P(None, 'tp'), may hold values from -4 to 4
- w_value: bfloat16 [2048, 2048], P(None, 'tp'), may hold values from -0.125 to 0.125
- w_outer: bfloat16 [2048, 2048], P(None, 'tp'), may hold values from -0.125 to 0.125
- w_inner: bfloat16 [2048, 2048], P(None, 'tp'), may hold values from -0.125 to 0.125
- w_signal: bfloat16 [2048, 2048], P(None, 'tp'), may hold values from -0.125 to 0.125
- conv_taps: bfloat16 [3, 2048], P(None, 'tp'), may hold values from -3.5 to 3.5
- lambdas: float32 [8], P('tp'), may hold values from 0.3 to 0.8
- head_gain: float32 [256], replicated, may hold values from 0.1 to 1.9
- attend_proj: bfloat16 [2048, 2048], P('tp'), may hold values from -0.125 to 0.125
- convolve_proj: bfloat16 [2048, 2048], P('tp'), may hold values from -0.125 to 0.125
Outputs:
- mixed: bfloat16 [6144, 2048], P(('sp', 'tp'))
- row_lse: float32 [6144, 16], P('sp', 'tp')
The draws below stay inside these ranges and needn't reach their ends.
All inputs are finite; a program needn't handle non-finite values.
Results may differ from the reference program's by a relative error of at most 0.015.
Values may be sent and summed in bfloat16 or wider, within the bound.
A program may use at most 128 MiB of HBM per device.

```python
import math
import jax
import jax.numpy as jnp
from jax import lax

D = 2048
HEADS = 8
HEAD_DIM = 128
CONV = 2048
TOK_DEV = 768
TOKENS = 6144
N_TP = 4


def query_key_pair(key):
    width = 2 * HEADS * HEAD_DIM
    spread = 1.3 / math.sqrt(D)
    key_part = jax.random.normal(jax.random.fold_in(key, 701), (D, width), jnp.float32) * spread
    noise_part = jax.random.normal(jax.random.fold_in(key, 702), (D, width), jnp.float32) * spread
    query_part = noise_part
    return (jnp.clip(query_part, -4.0, 4.0), jnp.clip(key_part, -4.0, 4.0))


def draw_w_query(key, part):
    return query_key_pair(key)[0].astype(jnp.bfloat16)


def draw_w_key(key, part):
    return query_key_pair(key)[1].astype(jnp.bfloat16)


def level_of(rng, dims, cuts, least, top_value):
    def one(position, parts):
        heights = jax.random.uniform(jax.random.fold_in(jax.random.fold_in(rng, 6), position), (parts,), jnp.float32, least / len(cuts), top_value / len(cuts))
        return jnp.repeat(jnp.exp(heights), dims[position] // parts).reshape((-1,) + (1,) * (len(dims) - position - 1))

    loudness = one(*cuts[0])
    for cut in cuts[1:]:
        loudness = loudness * one(*cut)
    return loudness


def bell_draw(rng, shape, scale, limit, pieces=(), kind=jnp.bfloat16):
    level = level_of(rng, shape, pieces, -0.22, 0.18) if pieces else 1.0
    entries = jax.random.normal(rng, shape, jnp.float32) * scale * level
    return jnp.minimum(jnp.maximum(entries, -limit), limit).astype(kind)


def setup_inputs(seed: int = 0) -> dict:
    keys = jax.random.split(jax.random.key(seed), 14)
    return {
        "tokens": bell_draw(keys[0], (TOKENS, D), 1.0, 6.0, ((0, 8), (1, 4))),
        "norm_gain": jnp.clip(1.0 + 0.18 * jax.random.normal(keys[1], (D,), jnp.float32), 0.1, 1.9),
        "w_query": draw_w_query(jax.random.fold_in(keys[13], 71), 0),
        "w_key": draw_w_key(jax.random.fold_in(keys[13], 71), 0),
        "w_value": bell_draw(keys[4], (D, 2 * HEADS * HEAD_DIM), D ** -0.5, 0.125, ((1, 4),)),
        "w_outer": bell_draw(keys[5], (D, CONV), D ** -0.5, 0.125, ((1, 4),)),
        "w_inner": bell_draw(keys[6], (D, CONV), D ** -0.5, 0.125, ((1, 4),)),
        "w_signal": bell_draw(keys[7], (D, CONV), D ** -0.5, 0.125, ((1, 4),)),
        "conv_taps": bell_draw(keys[8], (3, CONV), 3 ** -0.5, 3.5, ((1, 4),)),
        "lambdas": jnp.clip(0.3 + 0.5 * jax.random.uniform(keys[9], (HEADS,), jnp.float32) ** level_of(keys[9], (HEADS,), ((0, 4),), -0.2, 0.2), 0.3, 0.8),
        "head_gain": jnp.clip(1.0 + 0.18 * jax.random.normal(keys[10], (2 * HEAD_DIM,), jnp.float32), 0.1, 1.9),
        "attend_proj": bell_draw(keys[11], (2 * HEADS * HEAD_DIM, D), (2 * HEADS * HEAD_DIM) ** -0.5, 0.125, ((0, 4),)),
        "convolve_proj": bell_draw(keys[12], (CONV, D), CONV ** -0.5, 0.125, ((0, 4),)),
    }


ROPE_BASE = 500000.0
NORM_EPS = 1e-05
HEAD_KEEP = 0.8
MASKED = -1e+30

def rotate(values_in, positions):
    half_width = values_in.shape[-1] // 2
    inverse = ROPE_BASE ** (-jnp.arange(half_width, dtype=jnp.float32) * 2.0 / values_in.shape[-1])
    angles = positions.astype(jnp.float32)[:, None] * inverse[None, :]
    cosine = jnp.cos(angles)[:, None, :]
    sine_part = jnp.sin(angles)[:, None, :]
    first_half = values_in[..., :half_width]
    second_half = values_in[..., half_width:]
    return jnp.concatenate([first_half * cosine - second_half * sine_part, second_half * cosine + first_half * sine_part], axis=-1)

def reference(tokens, norm_gain, w_query, w_key, w_value, w_outer, w_inner, w_signal, conv_taps, lambdas, head_gain, attend_proj, convolve_proj):
    row_count = tokens.shape[0]
    widened = tokens.astype(jnp.float32)
    scaled = (widened * norm_gain[None, :]).astype(jnp.bfloat16)
    inv_rms = lax.rsqrt(lax.optimization_barrier(jnp.mean(widened * widened, axis=1, keepdims=True)) + NORM_EPS)

    def project(weight):
        return inv_rms * jnp.dot(scaled, weight, preferred_element_type=jnp.float32)
    positions = jnp.arange(row_count, dtype=jnp.int32)
    queries = rotate(project(w_query).reshape(row_count, 2 * HEADS, HEAD_DIM), positions).astype(jnp.bfloat16)
    key_rows = rotate(project(w_key).reshape(row_count, 2 * HEADS, HEAD_DIM), positions).astype(jnp.bfloat16)
    value_rows = project(w_value).astype(jnp.bfloat16).reshape(row_count, HEADS, 2 * HEAD_DIM)
    block_count = row_count // TOK_DEV
    key_places = jnp.arange(row_count, dtype=jnp.int32)
    attended_heads = []
    lse_heads = []
    for head_index in range(HEADS):
        head_query = queries[:, 2 * head_index:2 * head_index + 2, :].astype(jnp.float32)
        head_key = key_rows[:, 2 * head_index:2 * head_index + 2, :].astype(jnp.float32)
        head_value = value_rows[:, head_index, :].astype(jnp.float32)
        head_lambda = lambdas[head_index]

        def one_block(block_index):
            first_row = block_index * TOK_DEV
            query_block = lax.dynamic_slice_in_dim(head_query, first_row, TOK_DEV, 0)
            scores = jnp.einsum('qjd,kjd->jqk', query_block, head_key) * HEAD_DIM ** (-0.5)
            query_places = first_row + jnp.arange(TOK_DEV, dtype=jnp.int32)
            allowed = key_places[None, :] <= query_places[:, None]
            scores = jnp.where(allowed[None], scores, MASKED)
            running_max = lax.optimization_barrier(jnp.max(scores, axis=2, keepdims=True))
            lifted = jnp.exp(scores - running_max)
            weight_sum = lax.optimization_barrier(jnp.sum(lifted, axis=2, keepdims=True))
            weights = lax.optimization_barrier((lifted / weight_sum).astype(jnp.bfloat16))
            mixed_pair = jnp.einsum('jqk,ke->jqe', weights.astype(jnp.float32), head_value)
            difference = mixed_pair[0] - head_lambda * mixed_pair[1]
            scale_back = lax.rsqrt(lax.optimization_barrier(jnp.mean(difference * difference, axis=1, keepdims=True)) + NORM_EPS)
            normed = (difference * scale_back * head_gain[None, :] * HEAD_KEEP).astype(jnp.bfloat16)
            log_sum = jnp.transpose((running_max + jnp.log(weight_sum))[:, :, 0], (1, 0))
            return (normed, log_sum)
        normed_blocks, lse_blocks = lax.map(one_block, jnp.arange(block_count, dtype=jnp.int32))
        attended_heads.append(normed_blocks.reshape(row_count, 2 * HEAD_DIM))
        lse_heads.append(lse_blocks.reshape(row_count, 2))
    attended = jnp.concatenate(attended_heads, axis=1)
    row_lse = jnp.concatenate(lse_heads, axis=1)
    product = project(w_inner) * project(w_signal)
    padded = jnp.concatenate([jnp.zeros((2, CONV), jnp.float32), product], axis=0)
    tap_values = conv_taps.astype(jnp.float32)
    smoothed = tap_values[0] * padded[:-2] + tap_values[1] * padded[1:-1] + tap_values[2] * padded[2:]
    convolved = (project(w_outer) * smoothed).astype(jnp.bfloat16)
    head_columns = HEADS // N_TP * 2 * HEAD_DIM
    channel_columns = CONV // N_TP
    summed = jnp.zeros((row_count, D), jnp.float32)
    for group_index in range(N_TP):
        head_lo = group_index * head_columns
        chan_lo = group_index * channel_columns
        partial_value = jnp.dot(attended[:, head_lo:head_lo + head_columns], attend_proj[head_lo:head_lo + head_columns], preferred_element_type=jnp.float32)
        partial_value = partial_value + jnp.dot(convolved[:, chan_lo:chan_lo + channel_columns], convolve_proj[chan_lo:chan_lo + channel_columns], preferred_element_type=jnp.float32)
        rounded = lax.optimization_barrier(partial_value.astype(jnp.bfloat16))
        summed = summed + rounded.astype(jnp.float32)
    return (summed.astype(jnp.bfloat16), row_lse)
```

```python
import functools
import math

import jax
import jax.numpy as jnp
import numpy as np
from jax import lax
from jax.experimental import pallas as pl
from jax.experimental.pallas import tpu as pltpu
from jax.sharding import PartitionSpec as P

ROPE_BASE = 500000.0
NORM_EPS = 1e-05
HEAD_KEEP = 0.8
MASKED = -1e30
LOG2E = math.log2(math.e)
MESH = pl.DeviceIdType.MESH
PIECES = 4


def partner(value, axis, stride):
    return lax.ppermute(value, axis, [(i, i ^ 1 << stride) for i in range(lax.axis_size(axis))])


def passed_along(value, axis, steps):
    count = lax.axis_size(axis)
    initial, last = (max(0, -steps), min(count, count - steps))
    return lax.ppermute(value, axis, [(source, source + steps) for source in range(initial, last)])


def rotate(values_in, positions):
    half_width = values_in.shape[-1] // 2
    inverse = ROPE_BASE ** (-jnp.arange(half_width, dtype=jnp.float32) * 2.0 / values_in.shape[-1])
    angles = positions.astype(jnp.float32)[:, None] * inverse[None, :]
    cosine = jnp.cos(angles)[:, None, :]
    sine_part = jnp.sin(angles)[:, None, :]
    first_half = values_in[..., :half_width]
    second_half = values_in[..., half_width:]
    return jnp.concatenate(
        [
            first_half * cosine - second_half * sine_part,
            second_half * cosine + first_half * sine_part,
        ],
        axis=-1,
    )


def absorb(state, queries, positions, key_block, value_block, first_key):
    running_max, weight_sum, weighted = state
    head_count = weighted.shape[0]
    block_rows = key_block.shape[0]
    scores = jnp.einsum("qgd,kgd->gqk", queries, key_block, preferred_element_type=jnp.float32)
    scores = scores * queries.shape[-1] ** (-0.5)
    key_places = first_key + jnp.arange(block_rows, dtype=jnp.int32)
    allowed = key_places[None, :] <= positions[:, None]
    scores = jnp.where(allowed[None], scores, MASKED)
    scores = scores.reshape(head_count, 2, positions.shape[0], block_rows)
    raised = jnp.maximum(running_max, jnp.max(scores, axis=3))
    factor = jnp.exp(running_max - raised)
    lifted = jnp.exp(scores - raised[..., None])
    weight_sum = factor * weight_sum + jnp.sum(lifted, axis=3)
    values_here = value_block.reshape(block_rows, head_count, -1)
    weighted = factor[..., None] * weighted + jnp.einsum(
        "hjqk,khe->hjqe",
        lifted.astype(jnp.bfloat16),
        values_here,
        preferred_element_type=jnp.float32,
    )
    return (raised, weight_sum, weighted)


def empty_state(head_count, rows, head_width):
    return (
        jnp.full((head_count, 2, rows), MASKED, jnp.float32),
        jnp.zeros((head_count, 2, rows), jnp.float32),
        jnp.zeros((head_count, 2, rows, 2 * head_width), jnp.float32),
    )


def finish(state, lambdas, head_gain):
    running_max, weight_sum, weighted = state
    head_count = weighted.shape[0]
    rows = weighted.shape[2]
    normalized = weighted / weight_sum[..., None]
    difference = normalized[:, 0] - lambdas[:, None, None] * normalized[:, 1]
    scale_back = lax.rsqrt(jnp.mean(difference * difference, axis=2, keepdims=True) + NORM_EPS)
    attended = (difference * scale_back * head_gain[None, None, :] * HEAD_KEEP).astype(jnp.bfloat16)
    attended = jnp.transpose(attended, (1, 0, 2)).reshape(rows, head_count * weighted.shape[3])
    row_lse = jnp.transpose(running_max + jnp.log(weight_sum), (2, 0, 1)).reshape(
        rows, 2 * head_count
    )
    return (attended, row_lse)


def project_kernel(scale, tok_ref, gain_ref, wq_ref, wk_ref, wv_ref, cos_ref, sin_ref, q_ref, kv_ref):
    heads, _, pair = q_ref.shape
    width = pair // 2
    widened = tok_ref[...].astype(jnp.float32)
    scaled = (widened * gain_ref[...]).astype(jnp.bfloat16)
    mean = jnp.sum(widened * widened, axis=1, keepdims=True) / widened.shape[1]
    inv_rms = lax.rsqrt(mean + NORM_EPS)
    cosine, sine = cos_ref[...], sin_ref[...]

    def rotary(x):
        return x * cosine + pltpu.roll(x, width // 2, 1) * sine

    q = jnp.dot(scaled, wq_ref[...], preferred_element_type=jnp.float32) * inv_rms
    k = jnp.dot(scaled, wk_ref[...], preferred_element_type=jnp.float32) * inv_rms
    v = jnp.dot(scaled, wv_ref[...], preferred_element_type=jnp.float32) * inv_rms
    for head in range(heads):
        for j in range(2):
            cols = slice((2 * head + j) * width, (2 * head + j + 1) * width)
            place = slice(j * width, (j + 1) * width)
            q_ref[head, :, place] = (rotary(q[:, cols]) * scale).astype(jnp.bfloat16)
            kv_ref[head, :, place] = rotary(k[:, cols]).astype(jnp.bfloat16)
        kv_ref[head, :, pair:] = v[:, head * pair : (head + 1) * pair].astype(jnp.bfloat16)


def project(tokens, norm_gain, w_query, w_key, w_value, positions, head_count, head_width):
    rows, model_width = tokens.shape
    half = head_width // 2
    inverse = ROPE_BASE ** (-jnp.arange(half, dtype=jnp.float32) * 2.0 / head_width)
    angles = positions.astype(jnp.float32)[:, None] * inverse[None, :]
    cosine, sine = jnp.cos(angles), jnp.sin(angles)
    cosine = jnp.concatenate([cosine, cosine], axis=1)
    sine = jnp.concatenate([-sine, sine], axis=1)
    pair = 2 * head_width
    block = rows // 3 if rows % 48 == 0 else rows
    whole = lambda shape: pl.BlockSpec(shape, lambda i: (0,) * len(shape))
    return pl.pallas_call(
        functools.partial(project_kernel, head_width ** (-0.5) * LOG2E),
        grid=(rows // block,),
        out_shape=(
            jax.ShapeDtypeStruct((head_count, rows, pair), jnp.bfloat16),
            jax.ShapeDtypeStruct((head_count, rows, 2 * pair), jnp.bfloat16),
        ),
        in_specs=[
            pl.BlockSpec((block, model_width), lambda i: (i, 0)),
            whole((1, model_width)),
            whole(w_query.shape),
            whole(w_key.shape),
            whole(w_value.shape),
            pl.BlockSpec((block, head_width), lambda i: (i, 0)),
            pl.BlockSpec((block, head_width), lambda i: (i, 0)),
        ],
        out_specs=(
            pl.BlockSpec((head_count, block, pair), lambda i: (0, i, 0)),
            pl.BlockSpec((head_count, block, 2 * pair), lambda i: (0, i, 0)),
        ),
        compiler_params=pltpu.CompilerParams(vmem_limit_bytes=48 * 2**20),
        cost_estimate=pl.CostEstimate(
            flops=6 * rows * model_width * w_query.shape[1],
            bytes_accessed=2 * (rows * model_width + 3 * w_query.size + 3 * rows * w_query.shape[1]),
            transcendentals=0,
        ),
        name="project_qkv",
    )(tokens, norm_gain[None, :], w_query, w_key, w_value, cosine, sine)


def attend_kernel(
    groups,
    block,
    q_pair,
    kv_pair,
    lambdas_ref,
    gain_ref,
    out_ref,
    lse_ref,
    kv_all,
    q_own,
    acc,
    top,
    total,
    local_sem,
    send_right,
    recv_sem,
    swap_send,
    swap_recv,
):
    sp = lax.axis_index("sp")
    tp = lax.axis_index("tp")
    g, y = sp // 2, sp % 2
    _, rows, pair = q_pair.shape
    width = pair // 2
    blocks = rows // block

    def at(group, place):
        return (2 * group + place, tp)

    loads = (
        pltpu.make_async_copy(kv_pair.at[y], kv_all.at[sp], local_sem.at[0]),
        pltpu.make_async_copy(q_pair.at[y], q_own.at[y], local_sem.at[1]),
    )
    for load in loads:
        load.start()
    barrier = pltpu.get_barrier_semaphore()
    pl.semaphore_signal(barrier, inc=1, device_id=at(g, 1 - y), device_id_type=MESH)

    @pl.when(g > 0)
    def _():
        pl.semaphore_signal(barrier, inc=1, device_id=at(g - 1, y), device_id_type=MESH)

    @pl.when(g < groups - 1)
    def _():
        pl.semaphore_signal(barrier, inc=1, device_id=at(g + 1, y), device_id_type=MESH)

    beside = jnp.where(g > 0, 1, 0) + jnp.where(g < groups - 1, 1, 0)
    pl.semaphore_wait(barrier, 1 + beside)

    def swap(source, target, index):
        return pltpu.make_async_remote_copy(
            src_ref=source,
            dst_ref=target,
            send_sem=swap_send.at[index],
            recv_sem=swap_recv.at[index],
            device_id=at(g, 1 - y),
            device_id_type=MESH,
        )

    swaps = (
        swap(kv_pair.at[1 - y], kv_all.at[sp], 0),
        swap(q_pair.at[1 - y], q_own.at[y], 1),
    )
    for one_swap in swaps:
        one_swap.start()
    loads[0].wait()

    def right(chunk):
        return pltpu.make_async_remote_copy(
            src_ref=kv_all.at[chunk],
            dst_ref=kv_all.at[chunk],
            send_sem=send_right.at[chunk],
            recv_sem=recv_sem.at[chunk],
            device_id=at(jnp.minimum(g + 1, groups - 1), y),
            device_id_type=MESH,
        )

    @pl.when(g < groups - 1)
    def _():
        right(sp).start()

    acc[...] = jnp.zeros_like(acc)
    total[...] = jnp.zeros_like(total)
    top[...] = jnp.full_like(top, MASKED)

    def update(r, j, start, scores, values):
        here = pl.ds(start, block)
        old = top[r, j, here, :]
        new = jnp.maximum(old, jnp.max(scores, axis=1, keepdims=True))
        shrink = jnp.exp2(old - new)
        lifted = jnp.exp2(scores - new[:, :1])
        top[r, j, here, :] = new
        total[r, j, here, :] = shrink * total[r, j, here, :] + jnp.sum(lifted, axis=1, keepdims=True)
        acc[r, j, here, :] = shrink[:, :1] * acc[r, j, here, :] + jnp.dot(
            lifted.astype(jnp.bfloat16), values, preferred_element_type=jnp.float32
        )

    def scores_of(r, j, start, chunk, length):
        cols = slice(j * width, (j + 1) * width)
        queries = q_own[r, pl.ds(start, block), cols]
        keys = kv_all[chunk, :length, cols]
        return lax.dot_general(
            queries, keys, (((1,), (1,)), ((), ())), preferred_element_type=jnp.float32
        )

    def process(r, chunk):
        q_chunk = 2 * g + r

        @pl.when(chunk < q_chunk)
        def _():
            def one(b, carry):
                start = pl.multiple_of(b * block, block)
                for j in range(2):
                    update(r, j, start, scores_of(r, j, start, chunk, rows), kv_all[chunk, :, pair:])
                return carry

            lax.fori_loop(0, blocks, one, 0)

        @pl.when(chunk == q_chunk)
        def _():
            for b in range(blocks):
                length = (b + 1) * block
                query_at = b * block + lax.broadcasted_iota(jnp.int32, (block, length), 0)
                key_at = lax.broadcasted_iota(jnp.int32, (block, length), 1)
                for j in range(2):
                    scores = scores_of(r, j, b * block, chunk, length)
                    scores = jnp.where(key_at <= query_at, scores, MASKED)
                    update(r, j, b * block, scores, kv_all[chunk, :length, pair:])

    loads[1].wait()
    swaps[0].wait()

    @pl.when(g < groups - 1)
    def _():
        right(2 * g + 1 - y).start()

    swaps[1].wait()

    def visit(i, carry):
        step, half = i // 2, i % 2
        group = g - step
        chunk = 2 * group + jnp.where(half == 0, y, 1 - y)

        @pl.when(step > 0)
        def _():
            right(chunk).wait_recv()

            @pl.when(g < groups - 1)
            def _():
                right(chunk).start()

        def each(r, inner):
            process(r, chunk)
            return inner

        lax.fori_loop(0, 2, each, 0)
        return carry

    lax.fori_loop(0, 2 * g + 2, visit, 0)

    lam = lambdas_ref[y]
    gain = gain_ref[...] * HEAD_KEEP

    def close(i, carry):
        r, start = i // blocks, pl.multiple_of((i % blocks) * block, block)
        here = pl.ds(start, block)
        sums = [total[r, j, here, :] for j in range(2)]
        parts = [acc[r, j, here, :] / sums[j][:, :1] for j in range(2)]
        difference = parts[0] - lam * parts[1]
        mean = jnp.mean(difference * difference, axis=1, keepdims=True)
        out_ref[r, here, :] = (difference * lax.rsqrt(mean + NORM_EPS) * gain).astype(jnp.bfloat16)
        lses = [top[r, j, here, :] * (1.0 / LOG2E) + jnp.log(sums[j]) for j in range(2)]
        lane = lax.broadcasted_iota(jnp.int32, lses[0].shape, 1)
        lse_ref[r, here, :] = jnp.where(lane == 0, lses[0], lses[1])
        return carry

    lax.fori_loop(0, 2 * blocks, close, 0)

    def drain(chunk, carry):
        right(chunk).wait_send()
        return carry

    @pl.when(g < groups - 1)
    def _():
        lax.fori_loop(0, 2 * g + 2, drain, 0)


def attend(groups, q_pair, kv_pair, lambdas, head_gain):
    _, rows, pair = q_pair.shape
    block = rows // 3 if rows % 48 == 0 else rows
    vmem = pl.BlockSpec(memory_space=pltpu.VMEM)
    anywhere = pl.BlockSpec(memory_space=pl.ANY)
    chunks = 2 * groups
    lanes = 128
    return pl.pallas_call(
        functools.partial(attend_kernel, groups, block),
        out_shape=(
            jax.ShapeDtypeStruct((2, rows, pair), jnp.bfloat16),
            jax.ShapeDtypeStruct((2, rows, lanes), jnp.float32),
        ),
        in_specs=[anywhere] * 2 + [pl.BlockSpec(memory_space=pltpu.SMEM), vmem],
        out_specs=(vmem, vmem),
        scratch_shapes=[
            pltpu.VMEM((chunks, rows, 2 * pair), jnp.bfloat16),
            pltpu.VMEM((2, rows, pair), jnp.bfloat16),
            pltpu.VMEM((2, 2, rows, pair), jnp.float32),
            pltpu.VMEM((2, 2, rows, lanes), jnp.float32),
            pltpu.VMEM((2, 2, rows, lanes), jnp.float32),
            pltpu.SemaphoreType.DMA((2,)),
            pltpu.SemaphoreType.DMA((chunks,)),
            pltpu.SemaphoreType.DMA((chunks,)),
            pltpu.SemaphoreType.DMA((2,)),
            pltpu.SemaphoreType.DMA((2,)),
        ],
        compiler_params=pltpu.CompilerParams(
            collective_id=0, has_side_effects=True, vmem_limit_bytes=56 * 2**20
        ),
        cost_estimate=pl.CostEstimate(
            flops=8 * chunks * rows * rows * 3 * pair // 4,
            bytes_accessed=8 * rows * pair,
            transcendentals=0,
        ),
        name="attend_line",
    )(q_pair, kv_pair, lambdas, head_gain[None, :])


def attention_by_head(tokens, norm_gain, w_query, w_key, w_value, lambdas, head_gain, positions):
    head_count = lambdas.shape[0]
    head_width = w_query.shape[1] // (2 * head_count)
    count = lax.axis_size("sp")
    groups = count // 2
    y = lax.axis_index("sp") % 2
    queries, key_values = project(
        tokens, norm_gain, w_query, w_key, w_value, positions, head_count, head_width
    )
    result, lse = attend(groups, queries, key_values, lambdas, head_gain)
    lse = lse[:, :, :2]
    at_first = y == 0
    crossed = partner(jnp.where(at_first, result[1], result[0]), "sp", 0)
    crossed_lse = partner(jnp.where(at_first, lse[1], lse[0]), "sp", 0)
    first = jnp.where(at_first, result[0], crossed)
    last = jnp.where(at_first, crossed, result[1])
    first_lse = jnp.where(at_first, lse[0], crossed_lse)
    last_lse = jnp.where(at_first, crossed_lse, lse[1])
    return (
        jnp.concatenate([first, last], axis=1),
        jnp.concatenate([first_lse, last_lse], axis=1),
    )


def table_of(rows, chunks, head_width):
    half = head_width // 2
    inverse = ROPE_BASE ** (-np.arange(half, dtype=np.float64) * 2.0 / head_width)
    def both(places):
        angles = places[:, None] * inverse[None, :]
        angles = np.concatenate([angles, angles], axis=1)
        return np.cos(angles).astype(np.float32), np.sin(angles).astype(np.float32)
    near = both(np.arange(rows, dtype=np.float64))
    far = both(np.arange(chunks, dtype=np.float64) * rows)
    return np.stack(near), np.stack(far, axis=1)


def layer_kernel(
    tokens, w_query, w_key, w_value, w_outer, w_inner, w_signal, near_in, wa_in, wc_in,
    gain_ref, far_ref, taps_ref, lam_ref, head_gain_ref,
    out_ref, lse_ref,
    tok, wqkv, wconv, wo, near, kv, q_all, q_stage, prod, gate, cv, cv_stage, att, att_stage,
    lse_in, lse_stage, lam_in, rs_in, rs_stage, rs_keep, acc, top, total,
    local_sem, tok_send, tok_recv, kv_to_p, kv_to_y, kv_to_z, kv_recv, q_send, q_recv,
    cv_send, cv_recv, edge_sem, att_send, att_recv, lse_send, lse_recv, wo_send, wo_recv,
    lam_sem, rs_send, rs_recv,
):
    s, t = lax.axis_index("sp"), lax.axis_index("tp")
    x, c = t // 2, t % 2
    y, zl, zh = s % 2, (s // 2) % 2, s // 4
    last = lax.axis_size("sp") - 1
    s1, s2, s4 = s + 1 - 2 * y, s + 2 - 4 * zl, s + 4 - 8 * zh
    s6 = s4 + 2 - 4 * zl
    t1, t2 = t + 1 - 2 * c, t + 2 - 4 * x
    owner = c == zl
    other = c != zl
    rows, width = tok.shape[1], tok.shape[2]
    block = tokens.shape[1]
    pieces = PIECES
    piece = rows // pieces
    pair = wqkv.shape[1] // 3
    hw = pair // 2
    halves = 2 * piece
    bf16, f32 = jnp.bfloat16, jnp.float32

    def remote(src, dst, ss, rs, dev):
        return pltpu.make_async_remote_copy(
            src_ref=src, dst_ref=dst, send_sem=ss, recv_sem=rs, device_id=dev, device_id_type=MESH
        )

    def span(p):
        return pl.ds(pl.multiple_of(p * piece, 16), piece)

    def cols(b):
        return pl.ds(pl.multiple_of(b * block, 128), block)

    own_cols = pl.ds(pl.multiple_of(zh * pair, 128), pair)
    loads = [
        pltpu.make_async_copy(tokens, tok.at[0, :, cols(t)], local_sem.at[0]),
        pltpu.make_async_copy(w_query.at[:, own_cols], wqkv.at[:, 0:pair], local_sem.at[1]),
        pltpu.make_async_copy(w_key.at[:, own_cols], wqkv.at[:, pair : 2 * pair], local_sem.at[2]),
        pltpu.make_async_copy(w_value.at[:, own_cols], wqkv.at[:, 2 * pair :], local_sem.at[3]),
        pltpu.make_async_copy(near_in, near, local_sem.at[4]),
        pltpu.make_async_copy(w_inner, wconv.at[0], local_sem.at[5]),
        pltpu.make_async_copy(w_signal, wconv.at[1], local_sem.at[6]),
        pltpu.make_async_copy(w_outer, wconv.at[2], local_sem.at[7]),
        pltpu.make_async_copy(wa_in, wo.at[c], local_sem.at[8]),
        pltpu.make_async_copy(wc_in, wo.at[2 + c], local_sem.at[9]),
    ]
    for load in loads:
        load.start()

    barrier = pltpu.get_barrier_semaphore()
    peers = [(s1, t), (s2, t), (s4, t), (s6, t), (s, t1), (s, t2), (s2, t1), (s4, t1), (s6, t1)]
    for peer in peers:
        pl.semaphore_signal(barrier, inc=1, device_id=peer, device_id_type=MESH)
    up_ok, down_ok = s < last, s > 0
    up, down = jnp.minimum(s + 1, last), jnp.maximum(s - 1, 0)

    @pl.when((y == 1) & up_ok)
    def _():
        pl.semaphore_signal(barrier, inc=1, device_id=(up, t), device_id_type=MESH)

    @pl.when((y == 0) & down_ok)
    def _():
        pl.semaphore_signal(barrier, inc=1, device_id=(down, t), device_id_type=MESH)

    across = jnp.where(y == 1, jnp.where(up_ok, 1, 0), jnp.where(down_ok, 1, 0))
    pl.semaphore_wait(barrier, len(peers) + across)

    def tok_at(k, p, b):
        return tok.at[k, span(p), cols(b)]

    def own_to_p(p):
        return remote(tokens.at[span(p)], tok_at(0, p, t), tok_send.at[0, p], tok_recv.at[0, 1, p], (s, t1))

    def own_to_x(p):
        return remote(tokens.at[span(p)], tok_at(0, p, t), tok_send.at[1, p], tok_recv.at[0, 2, p], (s, t2))

    def own_to_f(p):
        return remote(tokens.at[span(p)], tok_at(1, p, t), tok_send.at[2, p], tok_recv.at[1, 0, p], (s4, t))

    def mate_to_f(p):
        return remote(tok_at(0, p, t1), tok_at(1, p, t1), tok_send.at[3, p], tok_recv.at[1, 1, p], (s4, t))

    def cross_to_p(k, p):
        return remote(
            tok_at(k, p, t2), tok_at(k, p, t2), tok_send.at[4 + 4 * k, p], tok_recv.at[k, 3, p], (s, t1)
        )

    def far_to_p(p):
        return remote(tok_at(1, p, t), tok_at(1, p, t), tok_send.at[5, p], tok_recv.at[1, 1, p], (s, t1))

    def mate_back(p):
        return remote(tok_at(1, p, t1), tok_at(1, p, t1), tok_send.at[6, p], tok_recv.at[1, 0, p], (s, t1))

    def far_to_x(p):
        return remote(tok_at(1, p, t), tok_at(1, p, t), tok_send.at[7, p], tok_recv.at[1, 2, p], (s, t2))

    def tok_got(k, index, p):
        block_of = (t, t1, t2, t1 + t2 - t)[index]
        here = tok_at(k, p, block_of)
        remote(here, here, tok_send.at[0, p], tok_recv.at[k, index, p], (s, t1)).wait_recv()

    def each(n, body, start=0):
        def one(i, carry):
            body(i)
            return carry

        lax.fori_loop(start, n, one, 0)

    def first_sends(p):
        own_to_x(p).start()
        own_to_p(p).start()

    each(pieces, first_sends)
    lam_copy = remote(lam_ref, lam_in, lam_sem.at[0], lam_sem.at[1], (s, t1))
    lam_copy.start()

    def second_sends(p):
        tok_got(0, 1, p)

        @pl.when(owner)
        def _():
            own_to_f(p).start()
            mate_to_f(p).start()

    each(pieces, second_sends)
    wo_copies = (
        remote(wa_in, wo.at[c], wo_send.at[0], wo_recv.at[0], (s, t1)),
        remote(wc_in, wo.at[2 + c], wo_send.at[1], wo_recv.at[1], (s, t1)),
    )
    for one_copy in wo_copies:
        one_copy.start()

    acc[...] = jnp.zeros_like(acc)
    total[...] = jnp.zeros_like(total)
    top[...] = jnp.full_like(top, MASKED)
    for load in loads:
        load.wait()

    def made(k):
        return jnp.where(owner, 4 * k, 8 + k)

    def kv_at(slot, p):
        return kv.at[slot, span(p)]

    def kv_p(slot, p):
        return remote(kv_at(slot, p), kv_at(slot, p), kv_to_p.at[slot, p], kv_recv.at[slot, p], (s, t1))

    def kv_y(slot, p):
        return remote(
            kv_at(slot, p), kv_at(slot + 1, p), kv_to_y.at[slot // 2, p], kv_recv.at[slot + 1, p], (s1, t)
        )

    def kv_z(k, p):
        return remote(
            kv_at(8 + k, p), kv_at(4 * k + 2, p), kv_to_z.at[k, p], kv_recv.at[4 * k + 2, p], (s2, t)
        )

    def q_rows(p):
        return pl.ds(pl.multiple_of((p // 2) * piece, 16), piece)

    def q_home(k, p):
        return remote(
            q_stage.at[k, span(p)], q_all.at[2 * k, q_rows(p)], q_send.at[k, p],
            q_recv.at[2 * k, p // 2], (s, t1),
        )

    def q_away(k, p):
        return remote(
            q_stage.at[k, span(p)], q_all.at[2 * k + 1, q_rows(p)], q_send.at[k, p],
            q_recv.at[2 * k + 1, p // 2], (s2, 2 * x + p % 2),
        )

    def ship(k, p):
        @pl.when(owner)
        def _():
            kv_y(4 * k, p).start()
            kv_p(4 * k, p).start()

            @pl.when(p % 2 != c)
            def _():
                q_home(k, p).start()

        @pl.when(other)
        def _():
            kv_z(k, p).start()
            q_away(k, p).start()

    def take(slot, p):
        if slot % 4 == 0:
            @pl.when(other)
            def _():
                kv_p(slot, p).wait_recv()
        else:
            kv_p(slot, p).wait_recv()

            @pl.when(owner)
            def _():
                if slot % 2 == 0:
                    kv_y(slot, p).start()
                kv_p(slot, p).start()

    sign = jnp.where(lax.broadcasted_iota(jnp.int32, (1, hw), 1) < hw // 2, -1.0, 1.0)

    def scaled_of(k, p):
        widened = tok[k, span(p), :].astype(f32)
        scaled = (widened * gain_ref[...]).astype(bf16)
        mean = jnp.sum(widened * widened, axis=1, keepdims=True) / width
        return scaled, lax.rsqrt(mean + NORM_EPS)

    def project_qkv(k, p, scaled, inv_rms):
        chunk = s if k == 0 else s4
        near_cos, near_sin = near[0, span(p), :], near[1, span(p), :]
        far_cos, far_sin = far_ref[chunk, 0:1, :], far_ref[chunk, 1:2, :]
        cosine = far_cos * near_cos - far_sin * near_sin
        sine = (far_sin * near_cos + far_cos * near_sin) * sign

        def rotary(v):
            return v * cosine + pltpu.roll(v, hw // 2, 1) * sine

        out = jnp.dot(scaled, wqkv[...], preferred_element_type=f32) * inv_rms
        slot = made(k)
        factor = hw ** (-0.5) * LOG2E
        queries = [(rotary(out[:, j * hw : (j + 1) * hw]) * factor).astype(bf16) for j in range(2)]
        for j in range(2):
            place = slice(pair + j * hw, pair + (j + 1) * hw)
            kv[slot, span(p), j * hw : (j + 1) * hw] = rotary(out[:, place]).astype(bf16)
        kv[slot, span(p), pair:] = out[:, 2 * pair :].astype(bf16)
        stay = owner & (p % 2 == c)

        @pl.when(stay)
        def _():
            for j in range(2):
                q_all[2 * k, q_rows(p), j * hw : (j + 1) * hw] = queries[j]

        @pl.when(jnp.logical_not(stay))
        def _():
            for j in range(2):
                q_stage[k, span(p), j * hw : (j + 1) * hw] = queries[j]

    def own_piece(p):
        tok_got(0, 2, p)
        cross_to_p(0, p).start()
        tok_got(0, 3, p)
        scaled, inv_rms = scaled_of(0, p)
        project_qkv(0, p, scaled, inv_rms)
        inner = jnp.dot(scaled, wconv[0], preferred_element_type=f32) * inv_rms
        signal = jnp.dot(scaled, wconv[1], preferred_element_type=f32) * inv_rms
        prod[pl.ds(pl.multiple_of(8 + p * piece, 8), piece), :] = inner * signal
        gate[span(p), :] = jnp.dot(scaled, wconv[2], preferred_element_type=f32) * inv_rms
        ship(0, p)

    each(pieces, own_piece)

    edge = remote(prod.at[rows : rows + 8], prod.at[0:8], edge_sem.at[0], edge_sem.at[1], (up, t))

    def far_forward(p):
        @pl.when(owner)
        def _():
            tok_got(1, 0, p)
            far_to_x(p).start()
            far_to_p(p).start()
            tok_got(1, 1, p)
            mate_back(p).start()

        @pl.when(other)
        def _():
            tok_got(1, 0, p)
            far_to_x(p).start()
            tok_got(1, 1, p)

    far_forward(0)

    @pl.when(up_ok)
    def _():
        edge.start()

    def far_piece(p):
        @pl.when(p < pieces - 1)
        def _():
            far_forward(p + 1)

        tok_got(1, 2, p)
        cross_to_p(1, p).start()
        tok_got(1, 3, p)
        scaled, inv_rms = scaled_of(1, p)
        project_qkv(1, p, scaled, inv_rms)
        take(0, p)
        take(1, p)
        take(2, p)
        ship(1, p)

    each(pieces, far_piece)

    @pl.when(down_ok)
    def _():
        edge.wait_recv()

    @pl.when(jnp.logical_not(down_ok))
    def _():
        prod[0:8, :] = jnp.zeros((8, prod.shape[1]), f32)

    taps = taps_ref[...].astype(f32)
    for p in range(pieces):
        begin = 8 + p * piece
        smoothed = (
            taps[0:1] * prod[begin - 2 : begin - 2 + piece, :]
            + taps[1:2] * prod[begin - 1 : begin - 1 + piece, :]
            + taps[2:3] * prod[begin : begin + piece, :]
        )
        convolved = (gate[p * piece : (p + 1) * piece, :] * smoothed).astype(bf16)
        place = slice((p // 2) * piece, (p // 2 + 1) * piece)

        @pl.when(c == p % 2)
        def _():
            cv[c, place, :] = convolved

        @pl.when(c != p % 2)
        def _():
            cv_stage[place, :] = convolved

    def more(p):
        take(3, p)
        take(6, p)
        take(4, p)
        take(5, p)

    each(pieces, more)
    cv_copy = remote(cv_stage, cv.at[c], cv_send.at[0], cv_recv.at[0], (s, t1))
    cv_copy.start()

    def xor(a, b):
        return a + b - 2 * a * b

    def chunk_of(slot):
        return 4 * xor(zh, slot // 4) + 2 * xor(zl, (slot // 2) % 2) + xor(y, slot % 2)

    def update(jq, m, here, scores, values):
        old = top[jq, m, here, :]
        new = jnp.maximum(old, jnp.max(scores, axis=1, keepdims=True))
        shrink = jnp.exp2(old - new)
        lifted = jnp.exp2(scores - new[:, :1])
        top[jq, m, here, :] = new
        total[jq, m, here, :] = shrink * total[jq, m, here, :] + jnp.sum(lifted, axis=1, keepdims=True)
        acc[jq, m, here, :] = shrink[:, :1] * acc[jq, m, here, :] + jnp.dot(
            lifted.astype(bf16), values, preferred_element_type=f32
        )

    def scores_of(jq, m, here, slot, length):
        place = slice(m * hw, (m + 1) * hw)
        return lax.dot_general(
            q_all[jq, here, place], kv[slot, :length, place], (((1,), (1,)), ((), ())),
            preferred_element_type=f32,
        )

    def whole(jq, slot):
        def sub(i):
            here = pl.ds(pl.multiple_of(i * piece, 16), piece)
            for m in range(2):
                update(jq, m, here, scores_of(jq, m, here, slot, rows), kv[slot, :, pair:])

        each(2, sub)

    def diagonal(jq):
        slot = 2 * jq
        for i in range(2):
            here = slice(i * piece, (i + 1) * piece)
            length = (2 * i + 2) * piece
            query_at = (2 * i + c) * piece + lax.broadcasted_iota(jnp.int32, (piece, length), 0)
            key_at = lax.broadcasted_iota(jnp.int32, (piece, length), 1)
            for m in range(2):
                scores = scores_of(jq, m, here, slot, length)
                scores = jnp.where(key_at <= query_at, scores, MASKED)
                update(jq, m, here, scores, kv[slot, :length, pair:])

    def q_got(jq):
        def one(i):
            here = q_all.at[jq, q_rows(2 * i)]
            remote(here, here, q_send.at[0, 0], q_recv.at[jq, i], (s, t1)).wait_recv()

        if jq % 2 == 1:
            each(2, one)
        else:
            @pl.when(other)
            def _():
                each(2, one)

    q_got(0)
    q_got(1)

    def near_pair(n):
        jq, slot = n // 4, n % 4

        @pl.when(chunk_of(slot) < chunk_of(2 * jq))
        def _():
            whole(jq, slot)

    each(8, near_pair)
    each(2, diagonal)

    each(pieces, functools.partial(take, 7))
    q_got(2)
    q_got(3)

    def far_pair(n):
        jq, slot = n // 8, n % 8

        @pl.when((chunk_of(slot) < chunk_of(2 * jq)) & ((jq >= 2) | (slot >= 4)))
        def _():
            whole(jq, slot)

    each(32, far_pair)
    each(4, diagonal, start=2)

    lam_copy.wait_recv()
    lam = jnp.where(owner, lam_ref[zh, 0:1, 0:1], lam_in[zh, 0:1, 0:1])
    gain = head_gain_ref[...] * HEAD_KEEP
    home = 2 * zl + zh
    seats = (s, s2, s4, s6)

    def att_away(jq, i):
        part = pl.ds(pl.multiple_of(i * piece, 16), piece)
        return remote(
            att_stage.at[jq - 1, part], att.at[home, part], att_send.at[jq - 1, i],
            att_recv.at[jq - 1, i], (seats[jq], t),
        )

    def att_got(jq, i):
        part = pl.ds(pl.multiple_of(i * piece, 16), piece)
        here = att.at[0, part]
        remote(here, here, att_send.at[jq - 1, i], att_recv.at[jq - 1, i], (seats[jq], t)).wait_recv()

    def lse_away(jq):
        return remote(
            lse_stage.at[jq], lse_in.at[zh, c], lse_send.at[jq], lse_recv.at[zh, c],
            (seats[jq], 2 * x + zl),
        )

    for jq in (3, 2, 1, 0):
        for i in range(2):
            here = slice(i * piece, (i + 1) * piece)
            sums = [total[jq, m, here, :] for m in range(2)]
            parts = [acc[jq, m, here, :] / sums[m][:, :1] for m in range(2)]
            difference = parts[0] - lam * parts[1]
            mean = jnp.mean(difference * difference, axis=1, keepdims=True)
            result = (difference * lax.rsqrt(mean + NORM_EPS) * gain).astype(bf16)
            if jq == 0:
                att[home, here, :] = result
            else:
                att_stage[jq - 1, here, :] = result
        tops = [top[jq, m] * (1.0 / LOG2E) + jnp.log(total[jq, m]) for m in range(2)]
        lane = lax.broadcasted_iota(jnp.int32, tops[0].shape, 1)
        turned = jnp.where(lane == 0, tops[0], tops[1]).T[0:8, :]
        if jq == 0:
            @pl.when(owner)
            def _():
                lse_in[zh, c] = turned

            @pl.when(other)
            def _():
                lse_stage[jq] = turned
                lse_away(jq).start()
        else:
            lse_stage[jq] = turned
            for i in range(2):
                att_away(jq, i).start()
            lse_away(jq).start()

    for one_copy in wo_copies:
        one_copy.wait_recv()
    cv_copy.wait_recv()
    n_cols = rs_in.shape[0]
    step = rs_in.shape[2]

    def partial(i, n):
        part = pl.ds(pl.multiple_of(i * piece, 16), piece)
        out_cols = pl.ds(pl.multiple_of(n * step, 128), step)
        result = None
        for h in range(4):
            term = jnp.dot(
                att[h, part, :], wo[h // 2, (h % 2) * pair : (h % 2 + 1) * pair, out_cols],
                preferred_element_type=f32,
            )
            result = term if result is None else result + term
        for core in range(2):
            result = result + jnp.dot(cv[core, part, :], wo[2 + core, :, out_cols], preferred_element_type=f32)
        return result

    def rs_copy(n):
        return remote(rs_stage.at[n], rs_in.at[n], rs_send.at[n], rs_recv.at[n], (s, t2))

    for jq in (1, 2, 3):
        att_got(jq, 1 - x)

    def give(n):
        rs_stage[n] = partial(1 - x, n).astype(bf16)
        rs_copy(n).start()

    each(n_cols, give)
    for jq in (1, 2, 3):
        att_got(jq, x)

    def keep(n):
        rs_keep[n] = partial(x, n)

    each(n_cols, keep)

    def lse_got(hl, cc):
        here = lse_in.at[hl, cc]

        @pl.when(jnp.logical_not((zl == c) & (zh == hl) & (cc == c)))
        def _():
            remote(here, here, lse_send.at[0], lse_recv.at[hl, cc], (s, t1)).wait_recv()

    for hl in range(2):
        for cc in range(2):
            lse_got(hl, cc)
    lse_ref[...] = lse_in[...]

    for n in range(n_cols):
        rs_copy(n).wait_recv()
        out_ref[:, n * step : (n + 1) * step] = (rs_keep[n] + rs_in[n].astype(f32)).astype(bf16)

    lam_copy.wait_send()
    for one_copy in wo_copies:
        one_copy.wait_send()
    cv_copy.wait_send()

    @pl.when(up_ok)
    def _():
        edge.wait_send()

    def drain(p):
        own_to_p(p).wait_send()
        own_to_x(p).wait_send()
        far_to_x(p).wait_send()
        for k in range(2):
            cross_to_p(k, p).wait_send()

        @pl.when(owner)
        def _():
            own_to_f(p).wait_send()
            mate_to_f(p).wait_send()
            far_to_p(p).wait_send()
            mate_back(p).wait_send()
            for slot in range(8):
                kv_p(slot, p).wait_send()
                if slot % 2 == 0:
                    kv_y(slot, p).wait_send()
            for k in range(2):
                @pl.when(p % 2 != c)
                def _():
                    q_home(k, p).wait_send()

        @pl.when(other)
        def _():
            for k in range(2):
                kv_z(k, p).wait_send()
                q_away(k, p).wait_send()

    each(pieces, drain)
    for jq in (1, 2, 3):
        for i in range(2):
            att_away(jq, i).wait_send()
        lse_away(jq).wait_send()

    @pl.when(other)
    def _():
        lse_away(0).wait_send()

    each(n_cols, lambda n: rs_copy(n).wait_send())


def whole_layer(
    tokens, norm_gain, w_query, w_key, w_value, w_outer, w_inner, w_signal, conv_taps, lambdas,
    head_gain, attend_proj, convolve_proj,
):
    rows, block = tokens.shape
    width = norm_gain.shape[0]
    chunks = lax.axis_size("sp")
    head_count = lambdas.shape[0]
    pair = w_query.shape[1] // head_count
    channels = w_inner.shape[1]
    piece = rows // PIECES
    near, far = table_of(rows, chunks, pair // 2)
    n_cols = 4
    step = width // n_cols
    vmem = pl.BlockSpec(memory_space=pltpu.VMEM)
    anywhere = pl.BlockSpec(memory_space=pl.ANY)
    bf16, f32 = jnp.bfloat16, jnp.float32
    dma = pltpu.SemaphoreType.DMA
    lam = jnp.broadcast_to(lambdas[:, None, None], (head_count, 8, 128))
    mixed, lse = pl.pallas_call(
        layer_kernel,
        out_shape=(
            jax.ShapeDtypeStruct((piece, width), bf16),
            jax.ShapeDtypeStruct((2, 2, 8, 2 * piece), f32),
        ),
        in_specs=[anywhere] * 10 + [vmem] * 5,
        out_specs=(vmem, vmem),
        scratch_shapes=[
            pltpu.VMEM((2, rows, width), bf16),
            pltpu.VMEM((width, 3 * pair), bf16),
            pltpu.VMEM((3, width, channels), bf16),
            pltpu.VMEM((4, channels, width), bf16),
            pltpu.VMEM(near.shape, f32),
            pltpu.VMEM((10, rows, 2 * pair), bf16),
            pltpu.VMEM((4, 2 * piece, pair), bf16),
            pltpu.VMEM((2, rows, pair), bf16),
            pltpu.VMEM((rows + 8, channels), f32),
            pltpu.VMEM((rows, channels), f32),
            pltpu.VMEM((2, 2 * piece, channels), bf16),
            pltpu.VMEM((2 * piece, channels), bf16),
            pltpu.VMEM((4, 2 * piece, pair), bf16),
            pltpu.VMEM((3, 2 * piece, pair), bf16),
            pltpu.VMEM((2, 2, 8, 2 * piece), f32),
            pltpu.VMEM((4, 8, 2 * piece), f32),
            pltpu.VMEM((head_count, 8, 128), f32),
            pltpu.VMEM((n_cols, piece, step), bf16),
            pltpu.VMEM((n_cols, piece, step), bf16),
            pltpu.VMEM((n_cols, piece, step), f32),
            pltpu.VMEM((4, 2, 2 * piece, pair), f32),
            pltpu.VMEM((4, 2, 2 * piece, 128), f32),
            pltpu.VMEM((4, 2, 2 * piece, 128), f32),
            dma((10,)),
            dma((9, PIECES)),
            dma((2, 4, PIECES)),
            dma((8, PIECES)),
            dma((4, PIECES)),
            dma((2, PIECES)),
            dma((8, PIECES)),
            dma((2, PIECES)),
            dma((4, 2)),
            dma((1,)),
            dma((1,)),
            dma((2,)),
            dma((3, 2)),
            dma((3, 2)),
            dma((4,)),
            dma((2, 2)),
            dma((2,)),
            dma((2,)),
            dma((2,)),
            dma((n_cols,)),
            dma((n_cols,)),
        ],
        compiler_params=pltpu.CompilerParams(
            collective_id=0, has_side_effects=True, vmem_limit_bytes=63 * 2**20
        ),
        name="whole_layer",
    )(
        tokens, w_query, w_key, w_value, w_outer, w_inner, w_signal, jnp.asarray(near), attend_proj,
        convolve_proj, norm_gain[None, :], jnp.asarray(far), conv_taps, lam, head_gain[None, :],
    )
    lse = lse[:, :, :2].reshape(2, 2, 2, 2, piece)
    lse = jnp.transpose(lse, (3, 1, 4, 0, 2)).reshape(rows, 2 * head_count)
    return mixed, lse


def make_fold(groups, row_count, carry, pieces):
    key_piece, value_piece = pieces
    block_rows = min(key_piece.shape[0], row_count)
    shard_count = key_piece.shape[0] // block_rows

    def one_shard(inner_states, shard_index):
        first_key = shard_index * block_rows
        key_block = lax.dynamic_slice_in_dim(key_piece, shard_index * block_rows, block_rows, 0)
        value_block = lax.dynamic_slice_in_dim(value_piece, shard_index * block_rows, block_rows, 0)
        updated_states = []
        for given_state, group in zip(inner_states, groups):
            group_queries, group_places, group_last = group

            def take_block(given):
                return absorb(given, group_queries, group_places, key_block, value_block, first_key)

            def leave_block(given):
                return given

            updated_states.append(
                lax.cond(first_key < group_last, take_block, leave_block, given_state)
            )
        return (tuple(updated_states), None)

    carry, _ = lax.scan(one_shard, carry, jnp.arange(shard_count, dtype=jnp.int32))
    return carry


def attention_by_rows(query_sums, key_sums, value_sums, lambdas, head_gain, positions):
    row_count = query_sums.shape[0]
    head_count = lambdas.shape[0]
    head_width = query_sums.shape[1] // (2 * head_count)
    offset = lax.axis_index("sp") * row_count
    split = (row_count, 2 * head_count, head_width)
    queries = rotate(query_sums.reshape(split), positions).astype(jnp.bfloat16)
    key_rows = rotate(key_sums.reshape(split), positions).astype(jnp.bfloat16)
    value_rows = value_sums.astype(jnp.bfloat16)
    half_rows = row_count // 2
    bit_count = lax.axis_size("sp").bit_length() - 1
    handed = queries[half_rows:]
    for bit_index in range(bit_count):
        handed = partner(handed, "sp", bit_index)
    mirror = lax.axis_size("sp") - 1 - lax.axis_index("sp")
    mirror_start = mirror * row_count + half_rows
    mirror_places = mirror_start + jnp.arange(half_rows, dtype=jnp.int32)
    groups = (
        (queries[:half_rows], positions[:half_rows], offset + half_rows),
        (handed, mirror_places, mirror_start + half_rows),
    )
    initial = (
        empty_state(head_count, half_rows, head_width),
        empty_state(head_count, half_rows, head_width),
    )
    states = make_fold(
        groups,
        row_count,
        initial,
        (
            lax.all_gather(key_rows, "sp", axis=0, tiled=True),
            lax.all_gather(value_rows, "sp", axis=0, tiled=True),
        ),
    )
    own_attended, own_lse = finish(states[0], lambdas, head_gain)
    answer = finish(states[1], lambdas, head_gain)
    for bit_index in range(bit_count):
        answer = (
            partner(answer[0], "sp", bit_index),
            partner(answer[1].astype(jnp.bfloat16), "sp", bit_index).astype(jnp.float32),
        )
    attended = jnp.concatenate([own_attended, answer[0]], axis=0)
    row_lse = jnp.concatenate([own_lse, answer[1]], axis=0)
    return (attended, row_lse)


def per_device(
    tokens,
    norm_gain,
    w_query,
    w_key,
    w_value,
    w_outer,
    w_inner,
    w_signal,
    conv_taps,
    lambdas,
    head_gain,
    attend_proj,
    convolve_proj,
):
    row_count = tokens.shape[0]
    model_width = norm_gain.shape[0]
    head_count = lambdas.shape[0]
    head_width = w_query.shape[1] // (2 * head_count)
    count = lax.axis_size("sp")
    fits = count == 8 and lax.axis_size("tp") == 4 and head_count == 2 and head_width == 128
    if fits and row_count % (16 * PIECES) == 0 and w_inner.shape[1] == w_query.shape[1]:
        return whole_layer(
            tokens, norm_gain, w_query, w_key, w_value, w_outer, w_inner, w_signal, conv_taps,
            lambdas, head_gain, attend_proj, convolve_proj,
        )
    gathered = lax.all_gather(tokens, "tp", axis=1, tiled=True)
    widened = gathered.astype(jnp.float32)
    scaled = (widened * norm_gain[None, :]).astype(jnp.bfloat16)
    squares = jnp.sum(widened * widened, axis=1)
    inv_rms = lax.rsqrt(squares / model_width + NORM_EPS)[:, None]
    offset = lax.axis_index("sp") * row_count
    positions = offset + jnp.arange(row_count, dtype=jnp.int32)

    def product_of(weight):
        return inv_rms * jnp.dot(scaled, weight, preferred_element_type=jnp.float32)

    if head_count == 2 and head_width == 128 and count % 2 == 0:
        attended, row_lse = attention_by_head(
            gathered, norm_gain, w_query, w_key, w_value, lambdas, head_gain, positions
        )
    else:
        attended, row_lse = attention_by_rows(
            product_of(w_query),
            product_of(w_key),
            product_of(w_value),
            lambdas,
            head_gain,
            positions,
        )
    outer_gate = product_of(w_outer)
    product = product_of(w_inner) * product_of(w_signal)
    border = passed_along(product[row_count - 2 :], "sp", 1)
    padded = jnp.concatenate([border, product], axis=0)
    tap_values = conv_taps.astype(jnp.float32)
    smoothed = (
        tap_values[0] * padded[:-2] + tap_values[1] * padded[1:-1] + tap_values[2] * padded[2:]
    )
    convolved = (outer_gate * smoothed).astype(jnp.bfloat16)
    mixed = lax.psum_scatter(
        (
            jnp.dot(attended, attend_proj, preferred_element_type=jnp.float32)
            + jnp.dot(convolved, convolve_proj, preferred_element_type=jnp.float32)
        ).astype(jnp.bfloat16),
        "tp",
        scatter_dimension=0,
        tiled=True,
    )
    return (mixed, row_lse)


def solution(mesh):
    return jax.shard_map(
        per_device,
        mesh=mesh,
        in_specs=(
            P("sp", "tp"),
            P(),
            P(None, "tp"),
            P(None, "tp"),
            P(None, "tp"),
            P(None, "tp"),
            P(None, "tp"),
            P(None, "tp"),
            P(None, "tp"),
            P("tp"),
            P(),
            P("tp", None),
            P("tp", None),
        ),
        out_specs=(P(("sp", "tp"), None), P("sp", "tp")),
        check_vma=False,
    )
```

```python
import functools
import math

import jax
import jax.numpy as jnp
import numpy as np
from jax import lax
from jax.experimental import pallas as pl
from jax.experimental.pallas import tpu as pltpu
from jax.sharding import PartitionSpec as P

ROPE_BASE = 500000.0
NORM_EPS = 1e-05
HEAD_KEEP = 0.8
MASKED = -1e30
LOG2E = math.log2(math.e)
MESH = pl.DeviceIdType.MESH
PIECES = 4


def partner(value, axis, stride):
    return lax.ppermute(value, axis, [(i, i ^ 1 << stride) for i in range(lax.axis_size(axis))])


def passed_along(value, axis, steps):
    count = lax.axis_size(axis)
    initial, last = (max(0, -steps), min(count, count - steps))
    return lax.ppermute(value, axis, [(source, source + steps) for source in range(initial, last)])


def rotate(values_in, positions):
    half_width = values_in.shape[-1] // 2
    inverse = ROPE_BASE ** (-jnp.arange(half_width, dtype=jnp.float32) * 2.0 / values_in.shape[-1])
    angles = positions.astype(jnp.float32)[:, None] * inverse[None, :]
    cosine = jnp.cos(angles)[:, None, :]
    sine_part = jnp.sin(angles)[:, None, :]
    first_half = values_in[..., :half_width]
    second_half = values_in[..., half_width:]
    return jnp.concatenate(
        [
            first_half * cosine - second_half * sine_part,
            second_half * cosine + first_half * sine_part,
        ],
        axis=-1,
    )


def absorb(state, queries, positions, key_block, value_block, first_key):
    running_max, weight_sum, weighted = state
    head_count = weighted.shape[0]
    block_rows = key_block.shape[0]
    scores = jnp.einsum("qgd,kgd->gqk", queries, key_block, preferred_element_type=jnp.float32)
    scores = scores * queries.shape[-1] ** (-0.5)
    key_places = first_key + jnp.arange(block_rows, dtype=jnp.int32)
    allowed = key_places[None, :] <= positions[:, None]
    scores = jnp.where(allowed[None], scores, MASKED)
    scores = scores.reshape(head_count, 2, positions.shape[0], block_rows)
    raised = jnp.maximum(running_max, jnp.max(scores, axis=3))
    factor = jnp.exp(running_max - raised)
    lifted = jnp.exp(scores - raised[..., None])
    weight_sum = factor * weight_sum + jnp.sum(lifted, axis=3)
    values_here = value_block.reshape(block_rows, head_count, -1)
    weighted = factor[..., None] * weighted + jnp.einsum(
        "hjqk,khe->hjqe",
        lifted.astype(jnp.bfloat16),
        values_here,
        preferred_element_type=jnp.float32,
    )
    return (raised, weight_sum, weighted)


def empty_state(head_count, rows, head_width):
    return (
        jnp.full((head_count, 2, rows), MASKED, jnp.float32),
        jnp.zeros((head_count, 2, rows), jnp.float32),
        jnp.zeros((head_count, 2, rows, 2 * head_width), jnp.float32),
    )


def finish(state, lambdas, head_gain):
    running_max, weight_sum, weighted = state
    head_count = weighted.shape[0]
    rows = weighted.shape[2]
    normalized = weighted / weight_sum[..., None]
    difference = normalized[:, 0] - lambdas[:, None, None] * normalized[:, 1]
    scale_back = lax.rsqrt(jnp.mean(difference * difference, axis=2, keepdims=True) + NORM_EPS)
    attended = (difference * scale_back * head_gain[None, None, :] * HEAD_KEEP).astype(jnp.bfloat16)
    attended = jnp.transpose(attended, (1, 0, 2)).reshape(rows, head_count * weighted.shape[3])
    row_lse = jnp.transpose(running_max + jnp.log(weight_sum), (2, 0, 1)).reshape(
        rows, 2 * head_count
    )
    return (attended, row_lse)


def project_kernel(scale, tok_ref, gain_ref, wq_ref, wk_ref, wv_ref, cos_ref, sin_ref, q_ref, kv_ref):
    heads, _, pair = q_ref.shape
    width = pair // 2
    widened = tok_ref[...].astype(jnp.float32)
    scaled = (widened * gain_ref[...]).astype(jnp.bfloat16)
    mean = jnp.sum(widened * widened, axis=1, keepdims=True) / widened.shape[1]
    inv_rms = lax.rsqrt(mean + NORM_EPS)
    cosine, sine = cos_ref[...], sin_ref[...]

    def rotary(x):
        return x * cosine + pltpu.roll(x, width // 2, 1) * sine

    q = jnp.dot(scaled, wq_ref[...], preferred_element_type=jnp.float32) * inv_rms
    k = jnp.dot(scaled, wk_ref[...], preferred_element_type=jnp.float32) * inv_rms
    v = jnp.dot(scaled, wv_ref[...], preferred_element_type=jnp.float32) * inv_rms
    for head in range(heads):
        for j in range(2):
            cols = slice((2 * head + j) * width, (2 * head + j + 1) * width)
            place = slice(j * width, (j + 1) * width)
            q_ref[head, :, place] = (rotary(q[:, cols]) * scale).astype(jnp.bfloat16)
            kv_ref[head, :, place] = rotary(k[:, cols]).astype(jnp.bfloat16)
        kv_ref[head, :, pair:] = v[:, head * pair : (head + 1) * pair].astype(jnp.bfloat16)


def project(tokens, norm_gain, w_query, w_key, w_value, positions, head_count, head_width):
    rows, model_width = tokens.shape
    half = head_width // 2
    inverse = ROPE_BASE ** (-jnp.arange(half, dtype=jnp.float32) * 2.0 / head_width)
    angles = positions.astype(jnp.float32)[:, None] * inverse[None, :]
    cosine, sine = jnp.cos(angles), jnp.sin(angles)
    cosine = jnp.concatenate([cosine, cosine], axis=1)
    sine = jnp.concatenate([-sine, sine], axis=1)
    pair = 2 * head_width
    block = rows // 3 if rows % 48 == 0 else rows
    whole = lambda shape: pl.BlockSpec(shape, lambda i: (0,) * len(shape))
    return pl.pallas_call(
        functools.partial(project_kernel, head_width ** (-0.5) * LOG2E),
        grid=(rows // block,),
        out_shape=(
            jax.ShapeDtypeStruct((head_count, rows, pair), jnp.bfloat16),
            jax.ShapeDtypeStruct((head_count, rows, 2 * pair), jnp.bfloat16),
        ),
        in_specs=[
            pl.BlockSpec((block, model_width), lambda i: (i, 0)),
            whole((1, model_width)),
            whole(w_query.shape),
            whole(w_key.shape),
            whole(w_value.shape),
            pl.BlockSpec((block, head_width), lambda i: (i, 0)),
            pl.BlockSpec((block, head_width), lambda i: (i, 0)),
        ],
        out_specs=(
            pl.BlockSpec((head_count, block, pair), lambda i: (0, i, 0)),
            pl.BlockSpec((head_count, block, 2 * pair), lambda i: (0, i, 0)),
        ),
        compiler_params=pltpu.CompilerParams(vmem_limit_bytes=48 * 2**20),
        cost_estimate=pl.CostEstimate(
            flops=6 * rows * model_width * w_query.shape[1],
            bytes_accessed=2 * (rows * model_width + 3 * w_query.size + 3 * rows * w_query.shape[1]),
            transcendentals=0,
        ),
        name="project_qkv",
    )(tokens, norm_gain[None, :], w_query, w_key, w_value, cosine, sine)


def attend_kernel(
    groups,
    block,
    q_pair,
    kv_pair,
    lambdas_ref,
    gain_ref,
    out_ref,
    lse_ref,
    kv_all,
    q_own,
    acc,
    top,
    total,
    local_sem,
    send_right,
    recv_sem,
    swap_send,
    swap_recv,
):
    sp = lax.axis_index("sp")
    tp = lax.axis_index("tp")
    g, y = sp // 2, sp % 2
    _, rows, pair = q_pair.shape
    width = pair // 2
    blocks = rows // block

    def at(group, place):
        return (2 * group + place, tp)

    loads = (
        pltpu.make_async_copy(kv_pair.at[y], kv_all.at[sp], local_sem.at[0]),
        pltpu.make_async_copy(q_pair.at[y], q_own.at[y], local_sem.at[1]),
    )
    for load in loads:
        load.start()
    barrier = pltpu.get_barrier_semaphore()
    pl.semaphore_signal(barrier, inc=1, device_id=at(g, 1 - y), device_id_type=MESH)

    @pl.when(g > 0)
    def _():
        pl.semaphore_signal(barrier, inc=1, device_id=at(g - 1, y), device_id_type=MESH)

    @pl.when(g < groups - 1)
    def _():
        pl.semaphore_signal(barrier, inc=1, device_id=at(g + 1, y), device_id_type=MESH)

    beside = jnp.where(g > 0, 1, 0) + jnp.where(g < groups - 1, 1, 0)
    pl.semaphore_wait(barrier, 1 + beside)

    def swap(source, target, index):
        return pltpu.make_async_remote_copy(
            src_ref=source,
            dst_ref=target,
            send_sem=swap_send.at[index],
            recv_sem=swap_recv.at[index],
            device_id=at(g, 1 - y),
            device_id_type=MESH,
        )

    swaps = (
        swap(kv_pair.at[1 - y], kv_all.at[sp], 0),
        swap(q_pair.at[1 - y], q_own.at[y], 1),
    )
    for one_swap in swaps:
        one_swap.start()
    loads[0].wait()

    def right(chunk):
        return pltpu.make_async_remote_copy(
            src_ref=kv_all.at[chunk],
            dst_ref=kv_all.at[chunk],
            send_sem=send_right.at[chunk],
            recv_sem=recv_sem.at[chunk],
            device_id=at(jnp.minimum(g + 1, groups - 1), y),
            device_id_type=MESH,
        )

    @pl.when(g < groups - 1)
    def _():
        right(sp).start()

    acc[...] = jnp.zeros_like(acc)
    total[...] = jnp.zeros_like(total)
    top[...] = jnp.full_like(top, MASKED)

    def update(r, j, start, scores, values):
        here = pl.ds(start, block)
        old = top[r, j, here, :]
        new = jnp.maximum(old, jnp.max(scores, axis=1, keepdims=True))
        shrink = jnp.exp2(old - new)
        lifted = jnp.exp2(scores - new[:, :1])
        top[r, j, here, :] = new
        total[r, j, here, :] = shrink * total[r, j, here, :] + jnp.sum(lifted, axis=1, keepdims=True)
        acc[r, j, here, :] = shrink[:, :1] * acc[r, j, here, :] + jnp.dot(
            lifted.astype(jnp.bfloat16), values, preferred_element_type=jnp.float32
        )

    def scores_of(r, j, start, chunk, length):
        cols = slice(j * width, (j + 1) * width)
        queries = q_own[r, pl.ds(start, block), cols]
        keys = kv_all[chunk, :length, cols]
        return lax.dot_general(
            queries, keys, (((1,), (1,)), ((), ())), preferred_element_type=jnp.float32
        )

    def process(r, chunk):
        q_chunk = 2 * g + r

        @pl.when(chunk < q_chunk)
        def _():
            def one(b, carry):
                start = pl.multiple_of(b * block, block)
                for j in range(2):
                    update(r, j, start, scores_of(r, j, start, chunk, rows), kv_all[chunk, :, pair:])
                return carry

            lax.fori_loop(0, blocks, one, 0)

        @pl.when(chunk == q_chunk)
        def _():
            for b in range(blocks):
                length = (b + 1) * block
                query_at = b * block + lax.broadcasted_iota(jnp.int32, (block, length), 0)
                key_at = lax.broadcasted_iota(jnp.int32, (block, length), 1)
                for j in range(2):
                    scores = scores_of(r, j, b * block, chunk, length)
                    scores = jnp.where(key_at <= query_at, scores, MASKED)
                    update(r, j, b * block, scores, kv_all[chunk, :length, pair:])

    loads[1].wait()
    swaps[0].wait()

    @pl.when(g < groups - 1)
    def _():
        right(2 * g + 1 - y).start()

    swaps[1].wait()

    def visit(i, carry):
        step, half = i // 2, i % 2
        group = g - step
        chunk = 2 * group + jnp.where(half == 0, y, 1 - y)

        @pl.when(step > 0)
        def _():
            right(chunk).wait_recv()

            @pl.when(g < groups - 1)
            def _():
                right(chunk).start()

        def each(r, inner):
            process(r, chunk)
            return inner

        lax.fori_loop(0, 2, each, 0)
        return carry

    lax.fori_loop(0, 2 * g + 2, visit, 0)

    lam = lambdas_ref[y]
    gain = gain_ref[...] * HEAD_KEEP

    def close(i, carry):
        r, start = i // blocks, pl.multiple_of((i % blocks) * block, block)
        here = pl.ds(start, block)
        sums = [total[r, j, here, :] for j in range(2)]
        parts = [acc[r, j, here, :] / sums[j][:, :1] for j in range(2)]
        difference = parts[0] - lam * parts[1]
        mean = jnp.mean(difference * difference, axis=1, keepdims=True)
        out_ref[r, here, :] = (difference * lax.rsqrt(mean + NORM_EPS) * gain).astype(jnp.bfloat16)
        lses = [top[r, j, here, :] * (1.0 / LOG2E) + jnp.log(sums[j]) for j in range(2)]
        lane = lax.broadcasted_iota(jnp.int32, lses[0].shape, 1)
        lse_ref[r, here, :] = jnp.where(lane == 0, lses[0], lses[1])
        return carry

    lax.fori_loop(0, 2 * blocks, close, 0)

    def drain(chunk, carry):
        right(chunk).wait_send()
        return carry

    @pl.when(g < groups - 1)
    def _():
        lax.fori_loop(0, 2 * g + 2, drain, 0)


def attend(groups, q_pair, kv_pair, lambdas, head_gain):
    _, rows, pair = q_pair.shape
    block = rows // 3 if rows % 48 == 0 else rows
    vmem = pl.BlockSpec(memory_space=pltpu.VMEM)
    anywhere = pl.BlockSpec(memory_space=pl.ANY)
    chunks = 2 * groups
    lanes = 128
    return pl.pallas_call(
        functools.partial(attend_kernel, groups, block),
        out_shape=(
            jax.ShapeDtypeStruct((2, rows, pair), jnp.bfloat16),
            jax.ShapeDtypeStruct((2, rows, lanes), jnp.float32),
        ),
        in_specs=[anywhere] * 2 + [pl.BlockSpec(memory_space=pltpu.SMEM), vmem],
        out_specs=(vmem, vmem),
        scratch_shapes=[
            pltpu.VMEM((chunks, rows, 2 * pair), jnp.bfloat16),
            pltpu.VMEM((2, rows, pair), jnp.bfloat16),
            pltpu.VMEM((2, 2, rows, pair), jnp.float32),
            pltpu.VMEM((2, 2, rows, lanes), jnp.float32),
            pltpu.VMEM((2, 2, rows, lanes), jnp.float32),
            pltpu.SemaphoreType.DMA((2,)),
            pltpu.SemaphoreType.DMA((chunks,)),
            pltpu.SemaphoreType.DMA((chunks,)),
            pltpu.SemaphoreType.DMA((2,)),
            pltpu.SemaphoreType.DMA((2,)),
        ],
        compiler_params=pltpu.CompilerParams(
            collective_id=0, has_side_effects=True, vmem_limit_bytes=56 * 2**20
        ),
        cost_estimate=pl.CostEstimate(
            flops=8 * chunks * rows * rows * 3 * pair // 4,
            bytes_accessed=8 * rows * pair,
            transcendentals=0,
        ),
        name="attend_line",
    )(q_pair, kv_pair, lambdas, head_gain[None, :])


def attention_by_head(tokens, norm_gain, w_query, w_key, w_value, lambdas, head_gain, positions):
    head_count = lambdas.shape[0]
    head_width = w_query.shape[1] // (2 * head_count)
    count = lax.axis_size("sp")
    groups = count // 2
    y = lax.axis_index("sp") % 2
    queries, key_values = project(
        tokens, norm_gain, w_query, w_key, w_value, positions, head_count, head_width
    )
    result, lse = attend(groups, queries, key_values, lambdas, head_gain)
    lse = lse[:, :, :2]
    at_first = y == 0
    crossed = partner(jnp.where(at_first, result[1], result[0]), "sp", 0)
    crossed_lse = partner(jnp.where(at_first, lse[1], lse[0]), "sp", 0)
    first = jnp.where(at_first, result[0], crossed)
    last = jnp.where(at_first, crossed, result[1])
    first_lse = jnp.where(at_first, lse[0], crossed_lse)
    last_lse = jnp.where(at_first, crossed_lse, lse[1])
    return (
        jnp.concatenate([first, last], axis=1),
        jnp.concatenate([first_lse, last_lse], axis=1),
    )


def table_of(rows, chunks, head_width):
    half = head_width // 2
    inverse = ROPE_BASE ** (-np.arange(half, dtype=np.float64) * 2.0 / head_width)
    def both(places):
        angles = places[:, None] * inverse[None, :]
        angles = np.concatenate([angles, angles], axis=1)
        return np.cos(angles).astype(np.float32), np.sin(angles).astype(np.float32)
    near = both(np.arange(rows, dtype=np.float64))
    far = both(np.arange(chunks, dtype=np.float64) * rows)
    return np.stack(near), np.stack(far, axis=1)


def layer_kernel(
    tokens, w_query, w_key, w_value, w_outer, w_inner, w_signal, near_in, wa_in, wc_in,
    gain_ref, far_ref, taps_ref, lam_ref, head_gain_ref,
    out_ref, lse_ref,
    tok, wqkv, wconv, wo, near, kv, q_all, q_stage, prod, gate, cv, cv_stage, att, att_stage,
    lse_in, lse_stage, lam_stage, lam_in, rs_in, rs_stage, rs_keep, acc, top, total,
    local_sem, tok_send, tok_recv, kv_to_p, kv_to_y, kv_to_z, kv_recv, q_send, q_recv,
    cv_send, cv_recv, edge_sem, att_send, att_recv, lse_send, lse_recv, wo_send, wo_recv,
    lam_sem, rs_send, rs_recv,
):
    s, t = lax.axis_index("sp"), lax.axis_index("tp")
    x, c = t // 2, t % 2
    y, zl, zh = s % 2, (s // 2) % 2, s // 4
    last = lax.axis_size("sp") - 1
    s1, s2, s4 = s + 1 - 2 * y, s + 2 - 4 * zl, s + 4 - 8 * zh
    s6 = s4 + 2 - 4 * zl
    t1, t2 = t + 1 - 2 * c, t + 2 - 4 * x
    owner = c == zl
    other = c != zl
    rows, width = tok.shape[1], tok.shape[2]
    block = tokens.shape[1]
    pieces = PIECES
    piece = rows // pieces
    pair = wqkv.shape[1] // 3
    hw = pair // 2
    halves = 2 * piece
    bf16, f32 = jnp.bfloat16, jnp.float32

    def remote(src, dst, ss, rs, dev):
        return pltpu.make_async_remote_copy(
            src_ref=src, dst_ref=dst, send_sem=ss, recv_sem=rs, device_id=dev, device_id_type=MESH
        )

    def span(p):
        return pl.ds(pl.multiple_of(p * piece, 16), piece)

    def cols(b):
        return pl.ds(pl.multiple_of(b * block, 128), block)

    own_cols = pl.ds(pl.multiple_of(zh * pair, 128), pair)
    loads = [
        pltpu.make_async_copy(tokens, tok.at[0, :, cols(t)], local_sem.at[0]),
        pltpu.make_async_copy(w_query.at[:, own_cols], wqkv.at[:, 0:pair], local_sem.at[1]),
        pltpu.make_async_copy(w_key.at[:, own_cols], wqkv.at[:, pair : 2 * pair], local_sem.at[2]),
        pltpu.make_async_copy(w_value.at[:, own_cols], wqkv.at[:, 2 * pair :], local_sem.at[3]),
        pltpu.make_async_copy(near_in, near, local_sem.at[4]),
        pltpu.make_async_copy(w_inner, wconv.at[0], local_sem.at[5]),
        pltpu.make_async_copy(w_signal, wconv.at[1], local_sem.at[6]),
        pltpu.make_async_copy(w_outer, wconv.at[2], local_sem.at[7]),
        pltpu.make_async_copy(wa_in, wo.at[c], local_sem.at[8]),
        pltpu.make_async_copy(wc_in, wo.at[2 + c], local_sem.at[9]),
    ]
    for load in loads:
        load.start()

    for hl in range(2):
        lam_stage[hl] = jnp.full(lam_stage.shape[1:], lam_ref[hl], f32)

    barrier = pltpu.get_barrier_semaphore()
    peers = [(s1, t), (s2, t), (s4, t), (s6, t), (s, t1), (s, t2), (s2, t1), (s4, t1), (s6, t1)]
    for peer in peers:
        pl.semaphore_signal(barrier, inc=1, device_id=peer, device_id_type=MESH)
    up_ok, down_ok = s < last, s > 0
    up, down = jnp.minimum(s + 1, last), jnp.maximum(s - 1, 0)

    @pl.when((y == 1) & up_ok)
    def _():
        pl.semaphore_signal(barrier, inc=1, device_id=(up, t), device_id_type=MESH)

    @pl.when((y == 0) & down_ok)
    def _():
        pl.semaphore_signal(barrier, inc=1, device_id=(down, t), device_id_type=MESH)

    across = jnp.where(y == 1, jnp.where(up_ok, 1, 0), jnp.where(down_ok, 1, 0))
    pl.semaphore_wait(barrier, len(peers) + across)

    def tok_at(k, p, b):
        return tok.at[k, span(p), cols(b)]

    def own_to_p(p):
        return remote(tokens.at[span(p)], tok_at(0, p, t), tok_send.at[0, p], tok_recv.at[0, 1, p], (s, t1))

    def own_to_x(p):
        return remote(tokens.at[span(p)], tok_at(0, p, t), tok_send.at[1, p], tok_recv.at[0, 2, p], (s, t2))

    def own_to_f(p):
        return remote(tokens.at[span(p)], tok_at(1, p, t), tok_send.at[2, p], tok_recv.at[1, 0, p], (s4, t))

    def mate_to_f(p):
        return remote(tok_at(0, p, t1), tok_at(1, p, t1), tok_send.at[3, p], tok_recv.at[1, 1, p], (s4, t))

    def cross_to_p(k, p):
        return remote(
            tok_at(k, p, t2), tok_at(k, p, t2), tok_send.at[4 + 4 * k, p], tok_recv.at[k, 3, p], (s, t1)
        )

    def far_to_p(p):
        return remote(tok_at(1, p, t), tok_at(1, p, t), tok_send.at[5, p], tok_recv.at[1, 1, p], (s, t1))

    def mate_back(p):
        return remote(tok_at(1, p, t1), tok_at(1, p, t1), tok_send.at[6, p], tok_recv.at[1, 0, p], (s, t1))

    def far_to_x(p):
        return remote(tok_at(1, p, t), tok_at(1, p, t), tok_send.at[7, p], tok_recv.at[1, 2, p], (s, t2))

    def tok_got(k, index, p):
        block_of = (t, t1, t2, t1 + t2 - t)[index]
        here = tok_at(k, p, block_of)
        remote(here, here, tok_send.at[0, p], tok_recv.at[k, index, p], (s, t1)).wait_recv()

    def each(n, body, start=0):
        def one(i, carry):
            body(i)
            return carry

        lax.fori_loop(start, n, one, 0)

    def first_sends(p):
        own_to_x(p).start()
        own_to_p(p).start()

    each(pieces, first_sends)
    lam_copy = remote(lam_stage, lam_in, lam_sem.at[0], lam_sem.at[1], (s, t1))
    lam_copy.start()

    def to_f(p):
        @pl.when(owner)
        def _():
            own_to_f(p).start()
            mate_to_f(p).start()

    def second_sends(p):
        tok_got(0, 1, p)

        @pl.when(p < 2)
        def _():
            to_f(p)

    each(pieces, second_sends)
    wo_copies = (
        remote(wa_in, wo.at[c], wo_send.at[0], wo_recv.at[0], (s, t1)),
        remote(wc_in, wo.at[2 + c], wo_send.at[1], wo_recv.at[1], (s, t1)),
    )
    for one_copy in wo_copies:
        one_copy.start()

    acc[...] = jnp.zeros_like(acc)
    total[...] = jnp.zeros_like(total)
    top[...] = jnp.full_like(top, MASKED)
    for load in loads:
        load.wait()

    def made(k):
        return jnp.where(owner, 4 * k, 8 + k)

    def kv_at(slot, p):
        return kv.at[slot, span(p)]

    def kv_p(slot, p):
        return remote(kv_at(slot, p), kv_at(slot, p), kv_to_p.at[slot, p], kv_recv.at[slot, p], (s, t1))

    def kv_y(slot, p):
        return remote(
            kv_at(slot, p), kv_at(slot + 1, p), kv_to_y.at[slot // 2, p], kv_recv.at[slot + 1, p], (s1, t)
        )

    def kv_z(k, p):
        return remote(
            kv_at(8 + k, p), kv_at(4 * k + 2, p), kv_to_z.at[k, p], kv_recv.at[4 * k + 2, p], (s2, t)
        )

    def q_rows(p):
        return pl.ds(pl.multiple_of((p // 2) * piece, 16), piece)

    def q_home(k, p):
        return remote(
            q_stage.at[k, span(p)], q_all.at[2 * k, q_rows(p)], q_send.at[k, p],
            q_recv.at[2 * k, p // 2], (s, t1),
        )

    def q_away(k, p):
        return remote(
            q_stage.at[k, span(p)], q_all.at[2 * k + 1, q_rows(p)], q_send.at[k, p],
            q_recv.at[2 * k + 1, p // 2], (s2, 2 * x + p % 2),
        )

    def ship(k, p):
        @pl.when(owner)
        def _():
            kv_y(4 * k, p).start()
            kv_p(4 * k, p).start()

            @pl.when(p % 2 != c)
            def _():
                q_home(k, p).start()

        @pl.when(other)
        def _():
            kv_z(k, p).start()
            q_away(k, p).start()

    def pass_on(slot, p):
        @pl.when(owner)
        def _():
            kv_p(slot, p).wait_recv()
            if slot % 2 == 0:
                kv_y(slot, p).start()
            kv_p(slot, p).start()

    def need(slot, low=0, high=PIECES):
        @pl.when(other)
        def _():
            each(high, lambda p: kv_p(slot, p).wait_recv(), start=low)

    sign = jnp.where(lax.broadcasted_iota(jnp.int32, (1, hw), 1) < hw // 2, -1.0, 1.0)

    def scaled_of(k, p):
        widened = tok[k, span(p), :].astype(f32)
        scaled = (widened * gain_ref[...]).astype(bf16)
        mean = jnp.sum(widened * widened, axis=1, keepdims=True) / width
        return scaled, lax.rsqrt(mean + NORM_EPS)

    def project_qkv(k, p, scaled, inv_rms):
        chunk = s if k == 0 else s4
        near_cos, near_sin = near[0, span(p), :], near[1, span(p), :]
        far_cos, far_sin = far_ref[chunk, 0:1, :], far_ref[chunk, 1:2, :]
        cosine = far_cos * near_cos - far_sin * near_sin
        sine = (far_sin * near_cos + far_cos * near_sin) * sign

        def rotary(v):
            return v * cosine + pltpu.roll(v, hw // 2, 1) * sine

        out = jnp.dot(scaled, wqkv[...], preferred_element_type=f32) * inv_rms
        slot = made(k)
        factor = hw ** (-0.5) * LOG2E
        queries = [(rotary(out[:, j * hw : (j + 1) * hw]) * factor).astype(bf16) for j in range(2)]
        for j in range(2):
            place = slice(pair + j * hw, pair + (j + 1) * hw)
            kv[slot, span(p), j * hw : (j + 1) * hw] = rotary(out[:, place]).astype(bf16)
        kv[slot, span(p), pair:] = out[:, 2 * pair :].astype(bf16)
        stay = owner & (p % 2 == c)

        @pl.when(stay)
        def _():
            for j in range(2):
                q_all[2 * k, q_rows(p), j * hw : (j + 1) * hw] = queries[j]

        @pl.when(jnp.logical_not(stay))
        def _():
            for j in range(2):
                q_stage[k, span(p), j * hw : (j + 1) * hw] = queries[j]

    def fill(p):
        scaled, inv_rms = scaled_of(0, p)
        inner = jnp.dot(scaled, wconv[0], preferred_element_type=f32) * inv_rms
        signal = jnp.dot(scaled, wconv[1], preferred_element_type=f32) * inv_rms
        prod[pl.ds(pl.multiple_of(8 + p * piece, 8), piece), :] = inner * signal
        gate[span(p), :] = jnp.dot(scaled, wconv[2], preferred_element_type=f32) * inv_rms

    def cross(k, p):
        tok_got(k, 2, p)
        cross_to_p(k, p).start()

    def finish_piece(k, p):
        tok_got(k, 3, p)
        scaled, inv_rms = scaled_of(k, p)
        project_qkv(k, p, scaled, inv_rms)
        ship(k, p)

    def own_piece(p):
        @pl.when(p == pieces - 1)
        def _():
            to_f(2)

        cross(0, p)
        finish_piece(0, p)

    each(pieces, own_piece)

    edge = remote(prod.at[rows : rows + 8], prod.at[0:8], edge_sem.at[0], edge_sem.at[1], (up, t))

    def far_forward(p):
        @pl.when(owner)
        def _():
            tok_got(1, 0, p)
            far_to_x(p).start()
            far_to_p(p).start()
            tok_got(1, 1, p)
            mate_back(p).start()

        @pl.when(other)
        def _():
            tok_got(1, 0, p)
            far_to_x(p).start()
            tok_got(1, 1, p)

    def pass_all(slot, low=0, high=PIECES):
        each(high, functools.partial(pass_on, slot), start=low)

    def xor(a, b):
        return a + b - 2 * a * b

    def level_of(k):
        return 2 * xor(zh, k // 2) + xor(zl, k % 2)

    lanes = top.shape[3]

    def absorb(jq, here, keys, values, seen=None):
        new_top, lifted, olds = [], [], []
        for m in range(2):
            place = slice(m * hw, (m + 1) * hw)
            scores = lax.dot_general(
                q_all[jq, here, place], keys(place), (((1,), (1,)), ((), ())),
                preferred_element_type=f32,
            )
            if seen is not None:
                scores = jnp.where(seen, scores, MASKED)
            lifted.append(scores)
            olds.append(top[jq, m, here, :])
        count = lifted[0].shape[1] // lanes
        parts = [[v[:, n * lanes : (n + 1) * lanes] for n in range(count)] for v in lifted]
        for m in range(2):
            best = functools.reduce(jnp.maximum, parts[m])
            new_top.append(jnp.maximum(olds[m], jnp.max(best, axis=1, keepdims=True)))
        raised = [[jnp.exp2(v - new_top[m]) for v in parts[m]] for m in range(2)]
        shrink = [jnp.exp2(olds[m] - new_top[m]) for m in range(2)]
        sums = [shrink[m] * total[jq, m, here, :] + functools.reduce(jnp.add, raised[m]) for m in range(2)]
        block_values = values()
        added = [
            jnp.dot(
                jnp.concatenate([v.astype(bf16) for v in raised[m]], axis=1), block_values,
                preferred_element_type=f32,
            )
            for m in range(2)
        ]
        wide = [jnp.concatenate([shrink[m]] * (pair // lanes), axis=1) for m in range(2)]
        grown = [wide[m] * acc[jq, m, here, :] + added[m] for m in range(2)]
        for m in range(2):
            top[jq, m, here, :] = new_top[m]
            total[jq, m, here, :] = sums[m]
            acc[jq, m, here, :] = grown[m]

    def part_of(i):
        return pl.ds(pl.multiple_of(i * piece, 16), piece)

    def both(jq, i, kp, low=0, high=None):
        high = rows if high is None else high

        def keys(place):
            return kv[pl.ds(2 * kp, 2), low:high, place].reshape(2 * (high - low), hw)

        def values():
            return kv[pl.ds(2 * kp, 2), low:high, pair:].reshape(2 * (high - low), pair)

        absorb(jq, part_of(i), keys, values)

    def beside(jq, i):
        slot = 2 * jq + 1
        absorb(jq, part_of(i), lambda place: kv[slot, :, place], lambda: kv[slot, :, pair:])

    def diagonal(jq, i):
        slot = 2 * jq
        for half in range(2):
            @pl.when(i == half)
            def _():
                length = (2 * half + 2) * piece
                query_at = (2 * half + c) * piece + lax.broadcasted_iota(jnp.int32, (piece, length), 0)
                key_at = lax.broadcasted_iota(jnp.int32, (piece, length), 1)
                absorb(
                    jq, part_of(i), lambda place: kv[slot, :length, place],
                    lambda: kv[slot, :length, pair:], key_at <= query_at,
                )

    def q_got(jq, i):
        def one():
            here = q_all.at[jq, q_rows(2 * i)]
            remote(here, here, q_send.at[0, 0], q_recv.at[jq, i], (s, t1)).wait_recv()

        if jq % 2 == 1:
            one()
        else:
            pl.when(other)(one)

    far_forward(0)
    to_f(3)
    far_forward(1)
    fill(0)
    pass_all(1)
    cross(1, 0)

    def far_piece(p):
        finish_piece(1, p)

        @pl.when((p > 0) & (p < pieces - 1))
        def _():
            far_forward(p + 1)

        @pl.when(p == 1)
        def _():
            pass_all(2)

        @pl.when(p < pieces - 1)
        def _():
            fill(p + 1)

            @pl.when(p == 1)
            def _():
                need(0)
                q_got(0, 0)
                q_got(0, 1)
                each(2, lambda i: diagonal(0, i))

            cross(1, p + 1)

    each(pieces, far_piece)

    @pl.when(up_ok)
    def _():
        edge.start()

    half = pieces // 2
    pass_on(6, 0)
    pass_all(5, 0, 3)
    need(2)
    q_got(1, 0)
    q_got(1, 1)
    each(2, lambda i: diagonal(1, i))
    pass_on(6, 1)
    pass_all(3)

    def near_level(n):
        jq, i = n // 2, n % 2

        @pl.when(level_of(1 - jq) < level_of(jq))
        def _():
            both(jq, i, 1 - jq)

        @pl.when(y == 1)
        def _():
            beside(jq, i)

    need(1)
    need(3)
    each(4, near_level)
    pass_on(6, 2)
    pass_on(5, 3)
    pass_all(7, 0, half)
    for slot in (4, 5, 6, 7):
        need(slot, 0, half)
    q_got(2, 0)
    q_got(3, 0)

    @pl.when(zh == 1)
    def _():
        each(8, lambda n: both(n // 4, (n // 2) % 2, 2 + n % 2, 0, halves))

    @pl.when(zh == 0)
    def _():
        each(4, lambda n: both(2 + n // 2, 0, n % 2))

    pass_on(6, 3)
    pass_on(7, 2)

    @pl.when(down_ok)
    def _():
        edge.wait_recv()

    @pl.when(jnp.logical_not(down_ok))
    def _():
        prod[0:8, :] = jnp.zeros((8, prod.shape[1]), f32)

    taps = taps_ref[...].astype(f32)
    for p in range(pieces):
        begin = 8 + p * piece
        smoothed = (
            taps[0:1] * prod[begin - 2 : begin - 2 + piece, :]
            + taps[1:2] * prod[begin - 1 : begin - 1 + piece, :]
            + taps[2:3] * prod[begin : begin + piece, :]
        )
        convolved = (gate[p * piece : (p + 1) * piece, :] * smoothed).astype(bf16)
        place = slice((p // 2) * piece, (p // 2 + 1) * piece)

        @pl.when(c == p % 2)
        def _():
            cv[c, place, :] = convolved

        @pl.when(c != p % 2)
        def _():
            cv_stage[place, :] = convolved

    cv_copy = remote(cv_stage, cv.at[c], cv_send.at[0], cv_recv.at[0], (s, t1))
    cv_copy.start()

    pass_on(7, 3)
    for slot in (4, 5, 6, 7):
        need(slot, half)
    q_got(2, 1)
    q_got(3, 1)

    lam_copy.wait_recv()
    lam = jnp.where(owner, lam_stage[zh, 0:1, :], lam_in[zh, 0:1, :])
    lam = jnp.concatenate([lam] * (pair // lanes), axis=1)
    gain = head_gain_ref[...] * HEAD_KEEP
    home = 2 * zl + zh

    def seat(jq):
        return 2 * level_of(jq) + y

    def att_away(jq, i):
        return remote(
            att_stage.at[jq - 1, part_of(i)], att.at[home, part_of(i)], att_send.at[jq - 1, i],
            att_recv.at[jq - 1, i], (seat(jq), t),
        )

    def att_got(jq, i):
        here = att.at[0, part_of(i)]
        remote(here, here, att_send.at[jq - 1, i], att_recv.at[jq - 1, i], (seat(jq), t)).wait_recv()

    def lse_away(jq):
        return remote(
            lse_stage.at[jq], lse_in.at[zh, c], lse_send.at[jq], lse_recv.at[zh, c],
            (seat(jq), 2 * x + zl),
        )

    def close(jq, i):
        here = part_of(i)
        parts = [
            acc[jq, m, here, :] / jnp.sum(total[jq, m, here, :], axis=1, keepdims=True) for m in range(2)
        ]
        difference = parts[0] - lam * parts[1]
        mean = jnp.mean(difference * difference, axis=1, keepdims=True)
        result = (difference * lax.rsqrt(mean + NORM_EPS) * gain).astype(bf16)

        @pl.when(jq == 0)
        def _():
            att[home, here, :] = result

        @pl.when(jq > 0)
        def _():
            att_stage[jq - 1, here, :] = result
            att_away(jq, i).start()

    def one_slot(i, n):
        jq = jnp.where(n < 2, n + 2, 3 - n)

        def one_level(kp):
            @pl.when((level_of(kp) < level_of(jq)) & (jq >= 2) & ((kp >= 2) | (i == 1)))
            def _():
                both(jq, i, kp)

            @pl.when((level_of(kp) < level_of(jq)) & (jq < 2) & (kp >= 2))
            def _():
                both(jq, i, kp, halves, rows)

        each(4, one_level)

        @pl.when(jq >= 2)
        def _():
            @pl.when(y == 1)
            def _():
                beside(jq, i)

            diagonal(jq, i)

        close(jq, i)

    def one_job(n):
        @pl.when(n == 6)
        def _():
            cv_copy.wait_recv()
            for one_copy in wo_copies:
                one_copy.wait_recv()
            for jq in (1, 2, 3):
                att_got(jq, 1 - x)
            each(n_cols, give)

        one_slot(jnp.where(n < 4, 1 - x, x), n % 4)

    n_cols = rs_in.shape[0]
    step = rs_in.shape[2]

    def partial(i, n):
        part = pl.ds(pl.multiple_of(i * piece, 16), piece)
        out_cols = pl.ds(pl.multiple_of(n * step, 128), step)
        result = None
        for h in range(4):
            term = jnp.dot(
                att[h, part, :], wo[h // 2, (h % 2) * pair : (h % 2 + 1) * pair, out_cols],
                preferred_element_type=f32,
            )
            result = term if result is None else result + term
        for core in range(2):
            result = result + jnp.dot(cv[core, part, :], wo[2 + core, :, out_cols], preferred_element_type=f32)
        return result

    def rs_copy(n):
        return remote(rs_stage.at[n], rs_in.at[n], rs_send.at[n], rs_recv.at[n], (s, t2))

    def give(n):
        rs_stage[n] = partial(1 - x, n).astype(bf16)
        rs_copy(n).start()

    each(8, one_job)
    for jq in (1, 2, 3):
        att_got(jq, x)

    def keep(n):
        rs_keep[n] = partial(x, n)

    each(n_cols, keep)

    for jq in (3, 2, 1, 0):
        tops = [
            top[jq, m] * (1.0 / LOG2E) + jnp.log(jnp.sum(total[jq, m], axis=1, keepdims=True))
            for m in range(2)
        ]
        lane = lax.broadcasted_iota(jnp.int32, tops[0].shape, 1)
        turned = jnp.where(lane == 0, tops[0], tops[1]).T[0:8, :]
        if jq == 0:
            @pl.when(owner)
            def _():
                lse_in[zh, c] = turned

            @pl.when(other)
            def _():
                lse_stage[jq] = turned
                lse_away(jq).start()
        else:
            lse_stage[jq] = turned
            lse_away(jq).start()

    def lse_got(hl, cc):
        here = lse_in.at[hl, cc]

        @pl.when(jnp.logical_not((zl == c) & (zh == hl) & (cc == c)))
        def _():
            remote(here, here, lse_send.at[0], lse_recv.at[hl, cc], (s, t1)).wait_recv()

    for hl in range(2):
        for cc in range(2):
            lse_got(hl, cc)
    for cc in range(2):
        both_heads = jnp.concatenate(
            [lse_in[0, cc, 0:2], lse_in[1, cc, 0:2], jnp.zeros((lanes - 4, halves), f32)], axis=0
        ).T
        for i in range(2):
            begin = (2 * i + cc) * piece
            lse_ref[begin : begin + piece, :] = both_heads[i * piece : (i + 1) * piece, 0:4]

    for n in range(n_cols):
        rs_copy(n).wait_recv()
        out_ref[:, n * step : (n + 1) * step] = (rs_keep[n] + rs_in[n].astype(f32)).astype(bf16)

    lam_copy.wait_send()
    for one_copy in wo_copies:
        one_copy.wait_send()
    cv_copy.wait_send()

    @pl.when(up_ok)
    def _():
        edge.wait_send()

    def drain(p):
        own_to_p(p).wait_send()
        own_to_x(p).wait_send()
        far_to_x(p).wait_send()
        for k in range(2):
            cross_to_p(k, p).wait_send()

        @pl.when(owner)
        def _():
            own_to_f(p).wait_send()
            mate_to_f(p).wait_send()
            far_to_p(p).wait_send()
            mate_back(p).wait_send()
            for slot in range(8):
                kv_p(slot, p).wait_send()
                if slot % 2 == 0:
                    kv_y(slot, p).wait_send()
            for k in range(2):
                @pl.when(p % 2 != c)
                def _():
                    q_home(k, p).wait_send()

        @pl.when(other)
        def _():
            for k in range(2):
                kv_z(k, p).wait_send()
                q_away(k, p).wait_send()

    each(pieces, drain)
    for jq in (1, 2, 3):
        for i in range(2):
            att_away(jq, i).wait_send()
        lse_away(jq).wait_send()

    @pl.when(other)
    def _():
        lse_away(0).wait_send()

    each(n_cols, lambda n: rs_copy(n).wait_send())


def whole_layer(
    tokens, norm_gain, w_query, w_key, w_value, w_outer, w_inner, w_signal, conv_taps, lambdas,
    head_gain, attend_proj, convolve_proj,
):
    rows, block = tokens.shape
    width = norm_gain.shape[0]
    chunks = lax.axis_size("sp")
    head_count = lambdas.shape[0]
    pair = w_query.shape[1] // head_count
    channels = w_inner.shape[1]
    piece = rows // PIECES
    near, far = table_of(rows, chunks, pair // 2)
    n_cols = 4
    step = width // n_cols
    vmem = pl.BlockSpec(memory_space=pltpu.VMEM)
    anywhere = pl.BlockSpec(memory_space=pl.ANY)
    bf16, f32 = jnp.bfloat16, jnp.float32
    dma = pltpu.SemaphoreType.DMA
    mixed, lse = pl.pallas_call(
        layer_kernel,
        out_shape=(
            jax.ShapeDtypeStruct((piece, width), bf16),
            jax.ShapeDtypeStruct((rows, 2 * head_count), f32),
        ),
        in_specs=[anywhere] * 10 + [vmem] * 3 + [pl.BlockSpec(memory_space=pltpu.SMEM), vmem],
        out_specs=(vmem, vmem),
        scratch_shapes=[
            pltpu.VMEM((2, rows, width), bf16),
            pltpu.VMEM((width, 3 * pair), bf16),
            pltpu.VMEM((3, width, channels), bf16),
            pltpu.VMEM((4, channels, width), bf16),
            pltpu.VMEM(near.shape, f32),
            pltpu.VMEM((10, rows, 2 * pair), bf16),
            pltpu.VMEM((4, 2 * piece, pair), bf16),
            pltpu.VMEM((2, rows, pair), bf16),
            pltpu.VMEM((rows + 8, channels), f32),
            pltpu.VMEM((rows, channels), f32),
            pltpu.VMEM((2, 2 * piece, channels), bf16),
            pltpu.VMEM((2 * piece, channels), bf16),
            pltpu.VMEM((4, 2 * piece, pair), bf16),
            pltpu.VMEM((3, 2 * piece, pair), bf16),
            pltpu.VMEM((2, 2, 8, 2 * piece), f32),
            pltpu.VMEM((4, 8, 2 * piece), f32),
            pltpu.VMEM((head_count, 8, 128), f32),
            pltpu.VMEM((head_count, 8, 128), f32),
            pltpu.VMEM((n_cols, piece, step), bf16),
            pltpu.VMEM((n_cols, piece, step), bf16),
            pltpu.VMEM((n_cols, piece, step), f32),
            pltpu.VMEM((4, 2, 2 * piece, pair), f32),
            pltpu.VMEM((4, 2, 2 * piece, 128), f32),
            pltpu.VMEM((4, 2, 2 * piece, 128), f32),
            dma((10,)),
            dma((9, PIECES)),
            dma((2, 4, PIECES)),
            dma((8, PIECES)),
            dma((4, PIECES)),
            dma((2, PIECES)),
            dma((8, PIECES)),
            dma((2, PIECES)),
            dma((4, 2)),
            dma((1,)),
            dma((1,)),
            dma((2,)),
            dma((3, 2)),
            dma((3, 2)),
            dma((4,)),
            dma((2, 2)),
            dma((2,)),
            dma((2,)),
            dma((2,)),
            dma((n_cols,)),
            dma((n_cols,)),
        ],
        compiler_params=pltpu.CompilerParams(
            collective_id=0, has_side_effects=True, vmem_limit_bytes=63 * 2**20
        ),
        name="whole_layer",
    )(
        tokens, w_query, w_key, w_value, w_outer, w_inner, w_signal, jnp.asarray(near), attend_proj,
        convolve_proj, norm_gain[None, :], jnp.asarray(far), conv_taps, lambdas, head_gain[None, :],
    )
    return mixed, lse


def make_fold(groups, row_count, carry, pieces):
    key_piece, value_piece = pieces
    block_rows = min(key_piece.shape[0], row_count)
    shard_count = key_piece.shape[0] // block_rows

    def one_shard(inner_states, shard_index):
        first_key = shard_index * block_rows
        key_block = lax.dynamic_slice_in_dim(key_piece, shard_index * block_rows, block_rows, 0)
        value_block = lax.dynamic_slice_in_dim(value_piece, shard_index * block_rows, block_rows, 0)
        updated_states = []
        for given_state, group in zip(inner_states, groups):
            group_queries, group_places, group_last = group

            def take_block(given):
                return absorb(given, group_queries, group_places, key_block, value_block, first_key)

            def leave_block(given):
                return given

            updated_states.append(
                lax.cond(first_key < group_last, take_block, leave_block, given_state)
            )
        return (tuple(updated_states), None)

    carry, _ = lax.scan(one_shard, carry, jnp.arange(shard_count, dtype=jnp.int32))
    return carry


def attention_by_rows(query_sums, key_sums, value_sums, lambdas, head_gain, positions):
    row_count = query_sums.shape[0]
    head_count = lambdas.shape[0]
    head_width = query_sums.shape[1] // (2 * head_count)
    offset = lax.axis_index("sp") * row_count
    split = (row_count, 2 * head_count, head_width)
    queries = rotate(query_sums.reshape(split), positions).astype(jnp.bfloat16)
    key_rows = rotate(key_sums.reshape(split), positions).astype(jnp.bfloat16)
    value_rows = value_sums.astype(jnp.bfloat16)
    half_rows = row_count // 2
    bit_count = lax.axis_size("sp").bit_length() - 1
    handed = queries[half_rows:]
    for bit_index in range(bit_count):
        handed = partner(handed, "sp", bit_index)
    mirror = lax.axis_size("sp") - 1 - lax.axis_index("sp")
    mirror_start = mirror * row_count + half_rows
    mirror_places = mirror_start + jnp.arange(half_rows, dtype=jnp.int32)
    groups = (
        (queries[:half_rows], positions[:half_rows], offset + half_rows),
        (handed, mirror_places, mirror_start + half_rows),
    )
    initial = (
        empty_state(head_count, half_rows, head_width),
        empty_state(head_count, half_rows, head_width),
    )
    states = make_fold(
        groups,
        row_count,
        initial,
        (
            lax.all_gather(key_rows, "sp", axis=0, tiled=True),
            lax.all_gather(value_rows, "sp", axis=0, tiled=True),
        ),
    )
    own_attended, own_lse = finish(states[0], lambdas, head_gain)
    answer = finish(states[1], lambdas, head_gain)
    for bit_index in range(bit_count):
        answer = (
            partner(answer[0], "sp", bit_index),
            partner(answer[1].astype(jnp.bfloat16), "sp", bit_index).astype(jnp.float32),
        )
    attended = jnp.concatenate([own_attended, answer[0]], axis=0)
    row_lse = jnp.concatenate([own_lse, answer[1]], axis=0)
    return (attended, row_lse)


def per_device(
    tokens,
    norm_gain,
    w_query,
    w_key,
    w_value,
    w_outer,
    w_inner,
    w_signal,
    conv_taps,
    lambdas,
    head_gain,
    attend_proj,
    convolve_proj,
):
    row_count = tokens.shape[0]
    model_width = norm_gain.shape[0]
    head_count = lambdas.shape[0]
    head_width = w_query.shape[1] // (2 * head_count)
    count = lax.axis_size("sp")
    fits = count == 8 and lax.axis_size("tp") == 4 and head_count == 2 and head_width == 128
    if fits and row_count % (16 * PIECES) == 0 and w_inner.shape[1] == w_query.shape[1]:
        return whole_layer(
            tokens, norm_gain, w_query, w_key, w_value, w_outer, w_inner, w_signal, conv_taps,
            lambdas, head_gain, attend_proj, convolve_proj,
        )
    gathered = lax.all_gather(tokens, "tp", axis=1, tiled=True)
    widened = gathered.astype(jnp.float32)
    scaled = (widened * norm_gain[None, :]).astype(jnp.bfloat16)
    squares = jnp.sum(widened * widened, axis=1)
    inv_rms = lax.rsqrt(squares / model_width + NORM_EPS)[:, None]
    offset = lax.axis_index("sp") * row_count
    positions = offset + jnp.arange(row_count, dtype=jnp.int32)

    def product_of(weight):
        return inv_rms * jnp.dot(scaled, weight, preferred_element_type=jnp.float32)

    if head_count == 2 and head_width == 128 and count % 2 == 0:
        attended, row_lse = attention_by_head(
            gathered, norm_gain, w_query, w_key, w_value, lambdas, head_gain, positions
        )
    else:
        attended, row_lse = attention_by_rows(
            product_of(w_query),
            product_of(w_key),
            product_of(w_value),
            lambdas,
            head_gain,
            positions,
        )
    outer_gate = product_of(w_outer)
    product = product_of(w_inner) * product_of(w_signal)
    border = passed_along(product[row_count - 2 :], "sp", 1)
    padded = jnp.concatenate([border, product], axis=0)
    tap_values = conv_taps.astype(jnp.float32)
    smoothed = (
        tap_values[0] * padded[:-2] + tap_values[1] * padded[1:-1] + tap_values[2] * padded[2:]
    )
    convolved = (outer_gate * smoothed).astype(jnp.bfloat16)
    mixed = lax.psum_scatter(
        (
            jnp.dot(attended, attend_proj, preferred_element_type=jnp.float32)
            + jnp.dot(convolved, convolve_proj, preferred_element_type=jnp.float32)
        ).astype(jnp.bfloat16),
        "tp",
        scatter_dimension=0,
        tiled=True,
    )
    return (mixed, row_lse)


def solution(mesh):
    return jax.shard_map(
        per_device,
        mesh=mesh,
        in_specs=(
            P("sp", "tp"),
            P(),
            P(None, "tp"),
            P(None, "tp"),
            P(None, "tp"),
            P(None, "tp"),
            P(None, "tp"),
            P(None, "tp"),
            P(None, "tp"),
            P("tp"),
            P(),
            P("tp", None),
            P("tp", None),
        ),
        out_specs=(P(("sp", "tp"), None), P("sp", "tp")),
        check_vma=False,
    )
```

```python
import functools
import math

import jax
import jax.numpy as jnp
import numpy as np
from jax import lax
from jax.experimental import pallas as pl
from jax.experimental.pallas import tpu as pltpu
from jax.sharding import PartitionSpec as P

ROPE_BASE = 500000.0
NORM_EPS = 1e-05
HEAD_KEEP = 0.8
MASKED = -1e30
LOG2E = math.log2(math.e)
MESH = pl.DeviceIdType.MESH
PIECES = 4


def partner(value, axis, stride):
    return lax.ppermute(value, axis, [(i, i ^ 1 << stride) for i in range(lax.axis_size(axis))])


def passed_along(value, axis, steps):
    count = lax.axis_size(axis)
    initial, last = (max(0, -steps), min(count, count - steps))
    return lax.ppermute(value, axis, [(source, source + steps) for source in range(initial, last)])


def rotate(values_in, positions):
    half_width = values_in.shape[-1] // 2
    inverse = ROPE_BASE ** (-jnp.arange(half_width, dtype=jnp.float32) * 2.0 / values_in.shape[-1])
    angles = positions.astype(jnp.float32)[:, None] * inverse[None, :]
    cosine = jnp.cos(angles)[:, None, :]
    sine_part = jnp.sin(angles)[:, None, :]
    first_half = values_in[..., :half_width]
    second_half = values_in[..., half_width:]
    return jnp.concatenate(
        [
            first_half * cosine - second_half * sine_part,
            second_half * cosine + first_half * sine_part,
        ],
        axis=-1,
    )


def absorb(state, queries, positions, key_block, value_block, first_key):
    running_max, weight_sum, weighted = state
    head_count = weighted.shape[0]
    block_rows = key_block.shape[0]
    scores = jnp.einsum("qgd,kgd->gqk", queries, key_block, preferred_element_type=jnp.float32)
    scores = scores * queries.shape[-1] ** (-0.5)
    key_places = first_key + jnp.arange(block_rows, dtype=jnp.int32)
    allowed = key_places[None, :] <= positions[:, None]
    scores = jnp.where(allowed[None], scores, MASKED)
    scores = scores.reshape(head_count, 2, positions.shape[0], block_rows)
    raised = jnp.maximum(running_max, jnp.max(scores, axis=3))
    factor = jnp.exp(running_max - raised)
    lifted = jnp.exp(scores - raised[..., None])
    weight_sum = factor * weight_sum + jnp.sum(lifted, axis=3)
    values_here = value_block.reshape(block_rows, head_count, -1)
    weighted = factor[..., None] * weighted + jnp.einsum(
        "hjqk,khe->hjqe",
        lifted.astype(jnp.bfloat16),
        values_here,
        preferred_element_type=jnp.float32,
    )
    return (raised, weight_sum, weighted)


def empty_state(head_count, rows, head_width):
    return (
        jnp.full((head_count, 2, rows), MASKED, jnp.float32),
        jnp.zeros((head_count, 2, rows), jnp.float32),
        jnp.zeros((head_count, 2, rows, 2 * head_width), jnp.float32),
    )


def finish(state, lambdas, head_gain):
    running_max, weight_sum, weighted = state
    head_count = weighted.shape[0]
    rows = weighted.shape[2]
    normalized = weighted / weight_sum[..., None]
    difference = normalized[:, 0] - lambdas[:, None, None] * normalized[:, 1]
    scale_back = lax.rsqrt(jnp.mean(difference * difference, axis=2, keepdims=True) + NORM_EPS)
    attended = (difference * scale_back * head_gain[None, None, :] * HEAD_KEEP).astype(jnp.bfloat16)
    attended = jnp.transpose(attended, (1, 0, 2)).reshape(rows, head_count * weighted.shape[3])
    row_lse = jnp.transpose(running_max + jnp.log(weight_sum), (2, 0, 1)).reshape(
        rows, 2 * head_count
    )
    return (attended, row_lse)


def project_kernel(scale, tok_ref, gain_ref, wq_ref, wk_ref, wv_ref, cos_ref, sin_ref, q_ref, kv_ref):
    heads, _, pair = q_ref.shape
    width = pair // 2
    widened = tok_ref[...].astype(jnp.float32)
    scaled = (widened * gain_ref[...]).astype(jnp.bfloat16)
    mean = jnp.sum(widened * widened, axis=1, keepdims=True) / widened.shape[1]
    inv_rms = lax.rsqrt(mean + NORM_EPS)
    cosine, sine = cos_ref[...], sin_ref[...]

    def rotary(x):
        return x * cosine + pltpu.roll(x, width // 2, 1) * sine

    q = jnp.dot(scaled, wq_ref[...], preferred_element_type=jnp.float32) * inv_rms
    k = jnp.dot(scaled, wk_ref[...], preferred_element_type=jnp.float32) * inv_rms
    v = jnp.dot(scaled, wv_ref[...], preferred_element_type=jnp.float32) * inv_rms
    for head in range(heads):
        for j in range(2):
            cols = slice((2 * head + j) * width, (2 * head + j + 1) * width)
            place = slice(j * width, (j + 1) * width)
            q_ref[head, :, place] = (rotary(q[:, cols]) * scale).astype(jnp.bfloat16)
            kv_ref[head, :, place] = rotary(k[:, cols]).astype(jnp.bfloat16)
        kv_ref[head, :, pair:] = v[:, head * pair : (head + 1) * pair].astype(jnp.bfloat16)


def project(tokens, norm_gain, w_query, w_key, w_value, positions, head_count, head_width):
    rows, model_width = tokens.shape
    half = head_width // 2
    inverse = ROPE_BASE ** (-jnp.arange(half, dtype=jnp.float32) * 2.0 / head_width)
    angles = positions.astype(jnp.float32)[:, None] * inverse[None, :]
    cosine, sine = jnp.cos(angles), jnp.sin(angles)
    cosine = jnp.concatenate([cosine, cosine], axis=1)
    sine = jnp.concatenate([-sine, sine], axis=1)
    pair = 2 * head_width
    block = rows // 3 if rows % 48 == 0 else rows
    whole = lambda shape: pl.BlockSpec(shape, lambda i: (0,) * len(shape))
    return pl.pallas_call(
        functools.partial(project_kernel, head_width ** (-0.5) * LOG2E),
        grid=(rows // block,),
        out_shape=(
            jax.ShapeDtypeStruct((head_count, rows, pair), jnp.bfloat16),
            jax.ShapeDtypeStruct((head_count, rows, 2 * pair), jnp.bfloat16),
        ),
        in_specs=[
            pl.BlockSpec((block, model_width), lambda i: (i, 0)),
            whole((1, model_width)),
            whole(w_query.shape),
            whole(w_key.shape),
            whole(w_value.shape),
            pl.BlockSpec((block, head_width), lambda i: (i, 0)),
            pl.BlockSpec((block, head_width), lambda i: (i, 0)),
        ],
        out_specs=(
            pl.BlockSpec((head_count, block, pair), lambda i: (0, i, 0)),
            pl.BlockSpec((head_count, block, 2 * pair), lambda i: (0, i, 0)),
        ),
        compiler_params=pltpu.CompilerParams(vmem_limit_bytes=48 * 2**20),
        cost_estimate=pl.CostEstimate(
            flops=6 * rows * model_width * w_query.shape[1],
            bytes_accessed=2 * (rows * model_width + 3 * w_query.size + 3 * rows * w_query.shape[1]),
            transcendentals=0,
        ),
        name="project_qkv",
    )(tokens, norm_gain[None, :], w_query, w_key, w_value, cosine, sine)


def attend_kernel(
    groups,
    block,
    q_pair,
    kv_pair,
    lambdas_ref,
    gain_ref,
    out_ref,
    lse_ref,
    kv_all,
    q_own,
    acc,
    top,
    total,
    local_sem,
    send_right,
    recv_sem,
    swap_send,
    swap_recv,
):
    sp = lax.axis_index("sp")
    tp = lax.axis_index("tp")
    g, y = sp // 2, sp % 2
    _, rows, pair = q_pair.shape
    width = pair // 2
    blocks = rows // block

    def at(group, place):
        return (2 * group + place, tp)

    loads = (
        pltpu.make_async_copy(kv_pair.at[y], kv_all.at[sp], local_sem.at[0]),
        pltpu.make_async_copy(q_pair.at[y], q_own.at[y], local_sem.at[1]),
    )
    for load in loads:
        load.start()
    barrier = pltpu.get_barrier_semaphore()
    pl.semaphore_signal(barrier, inc=1, device_id=at(g, 1 - y), device_id_type=MESH)

    @pl.when(g > 0)
    def _():
        pl.semaphore_signal(barrier, inc=1, device_id=at(g - 1, y), device_id_type=MESH)

    @pl.when(g < groups - 1)
    def _():
        pl.semaphore_signal(barrier, inc=1, device_id=at(g + 1, y), device_id_type=MESH)

    beside = jnp.where(g > 0, 1, 0) + jnp.where(g < groups - 1, 1, 0)
    pl.semaphore_wait(barrier, 1 + beside)

    def swap(source, target, index):
        return pltpu.make_async_remote_copy(
            src_ref=source,
            dst_ref=target,
            send_sem=swap_send.at[index],
            recv_sem=swap_recv.at[index],
            device_id=at(g, 1 - y),
            device_id_type=MESH,
        )

    swaps = (
        swap(kv_pair.at[1 - y], kv_all.at[sp], 0),
        swap(q_pair.at[1 - y], q_own.at[y], 1),
    )
    for one_swap in swaps:
        one_swap.start()
    loads[0].wait()

    def right(chunk):
        return pltpu.make_async_remote_copy(
            src_ref=kv_all.at[chunk],
            dst_ref=kv_all.at[chunk],
            send_sem=send_right.at[chunk],
            recv_sem=recv_sem.at[chunk],
            device_id=at(jnp.minimum(g + 1, groups - 1), y),
            device_id_type=MESH,
        )

    @pl.when(g < groups - 1)
    def _():
        right(sp).start()

    acc[...] = jnp.zeros_like(acc)
    total[...] = jnp.zeros_like(total)
    top[...] = jnp.full_like(top, MASKED)

    def update(r, j, start, scores, values):
        here = pl.ds(start, block)
        old = top[r, j, here, :]
        new = jnp.maximum(old, jnp.max(scores, axis=1, keepdims=True))
        shrink = jnp.exp2(old - new)
        lifted = jnp.exp2(scores - new[:, :1])
        top[r, j, here, :] = new
        total[r, j, here, :] = shrink * total[r, j, here, :] + jnp.sum(lifted, axis=1, keepdims=True)
        acc[r, j, here, :] = shrink[:, :1] * acc[r, j, here, :] + jnp.dot(
            lifted.astype(jnp.bfloat16), values, preferred_element_type=jnp.float32
        )

    def scores_of(r, j, start, chunk, length):
        cols = slice(j * width, (j + 1) * width)
        queries = q_own[r, pl.ds(start, block), cols]
        keys = kv_all[chunk, :length, cols]
        return lax.dot_general(
            queries, keys, (((1,), (1,)), ((), ())), preferred_element_type=jnp.float32
        )

    def process(r, chunk):
        q_chunk = 2 * g + r

        @pl.when(chunk < q_chunk)
        def _():
            def one(b, carry):
                start = pl.multiple_of(b * block, block)
                for j in range(2):
                    update(r, j, start, scores_of(r, j, start, chunk, rows), kv_all[chunk, :, pair:])
                return carry

            lax.fori_loop(0, blocks, one, 0)

        @pl.when(chunk == q_chunk)
        def _():
            for b in range(blocks):
                length = (b + 1) * block
                query_at = b * block + lax.broadcasted_iota(jnp.int32, (block, length), 0)
                key_at = lax.broadcasted_iota(jnp.int32, (block, length), 1)
                for j in range(2):
                    scores = scores_of(r, j, b * block, chunk, length)
                    scores = jnp.where(key_at <= query_at, scores, MASKED)
                    update(r, j, b * block, scores, kv_all[chunk, :length, pair:])

    loads[1].wait()
    swaps[0].wait()

    @pl.when(g < groups - 1)
    def _():
        right(2 * g + 1 - y).start()

    swaps[1].wait()

    def visit(i, carry):
        step, half = i // 2, i % 2
        group = g - step
        chunk = 2 * group + jnp.where(half == 0, y, 1 - y)

        @pl.when(step > 0)
        def _():
            right(chunk).wait_recv()

            @pl.when(g < groups - 1)
            def _():
                right(chunk).start()

        def each(r, inner):
            process(r, chunk)
            return inner

        lax.fori_loop(0, 2, each, 0)
        return carry

    lax.fori_loop(0, 2 * g + 2, visit, 0)

    lam = lambdas_ref[y]
    gain = gain_ref[...] * HEAD_KEEP

    def close(i, carry):
        r, start = i // blocks, pl.multiple_of((i % blocks) * block, block)
        here = pl.ds(start, block)
        sums = [total[r, j, here, :] for j in range(2)]
        parts = [acc[r, j, here, :] / sums[j][:, :1] for j in range(2)]
        difference = parts[0] - lam * parts[1]
        mean = jnp.mean(difference * difference, axis=1, keepdims=True)
        out_ref[r, here, :] = (difference * lax.rsqrt(mean + NORM_EPS) * gain).astype(jnp.bfloat16)
        lses = [top[r, j, here, :] * (1.0 / LOG2E) + jnp.log(sums[j]) for j in range(2)]
        lane = lax.broadcasted_iota(jnp.int32, lses[0].shape, 1)
        lse_ref[r, here, :] = jnp.where(lane == 0, lses[0], lses[1])
        return carry

    lax.fori_loop(0, 2 * blocks, close, 0)

    def drain(chunk, carry):
        right(chunk).wait_send()
        return carry

    @pl.when(g < groups - 1)
    def _():
        lax.fori_loop(0, 2 * g + 2, drain, 0)


def attend(groups, q_pair, kv_pair, lambdas, head_gain):
    _, rows, pair = q_pair.shape
    block = rows // 3 if rows % 48 == 0 else rows
    vmem = pl.BlockSpec(memory_space=pltpu.VMEM)
    anywhere = pl.BlockSpec(memory_space=pl.ANY)
    chunks = 2 * groups
    lanes = 128
    return pl.pallas_call(
        functools.partial(attend_kernel, groups, block),
        out_shape=(
            jax.ShapeDtypeStruct((2, rows, pair), jnp.bfloat16),
            jax.ShapeDtypeStruct((2, rows, lanes), jnp.float32),
        ),
        in_specs=[anywhere] * 2 + [pl.BlockSpec(memory_space=pltpu.SMEM), vmem],
        out_specs=(vmem, vmem),
        scratch_shapes=[
            pltpu.VMEM((chunks, rows, 2 * pair), jnp.bfloat16),
            pltpu.VMEM((2, rows, pair), jnp.bfloat16),
            pltpu.VMEM((2, 2, rows, pair), jnp.float32),
            pltpu.VMEM((2, 2, rows, lanes), jnp.float32),
            pltpu.VMEM((2, 2, rows, lanes), jnp.float32),
            pltpu.SemaphoreType.DMA((2,)),
            pltpu.SemaphoreType.DMA((chunks,)),
            pltpu.SemaphoreType.DMA((chunks,)),
            pltpu.SemaphoreType.DMA((2,)),
            pltpu.SemaphoreType.DMA((2,)),
        ],
        compiler_params=pltpu.CompilerParams(
            collective_id=0, has_side_effects=True, vmem_limit_bytes=56 * 2**20
        ),
        cost_estimate=pl.CostEstimate(
            flops=8 * chunks * rows * rows * 3 * pair // 4,
            bytes_accessed=8 * rows * pair,
            transcendentals=0,
        ),
        name="attend_line",
    )(q_pair, kv_pair, lambdas, head_gain[None, :])


def attention_by_head(tokens, norm_gain, w_query, w_key, w_value, lambdas, head_gain, positions):
    head_count = lambdas.shape[0]
    head_width = w_query.shape[1] // (2 * head_count)
    count = lax.axis_size("sp")
    groups = count // 2
    y = lax.axis_index("sp") % 2
    queries, key_values = project(
        tokens, norm_gain, w_query, w_key, w_value, positions, head_count, head_width
    )
    result, lse = attend(groups, queries, key_values, lambdas, head_gain)
    lse = lse[:, :, :2]
    at_first = y == 0
    crossed = partner(jnp.where(at_first, result[1], result[0]), "sp", 0)
    crossed_lse = partner(jnp.where(at_first, lse[1], lse[0]), "sp", 0)
    first = jnp.where(at_first, result[0], crossed)
    last = jnp.where(at_first, crossed, result[1])
    first_lse = jnp.where(at_first, lse[0], crossed_lse)
    last_lse = jnp.where(at_first, crossed_lse, lse[1])
    return (
        jnp.concatenate([first, last], axis=1),
        jnp.concatenate([first_lse, last_lse], axis=1),
    )


def table_of(rows, chunks, head_width):
    half = head_width // 2
    inverse = ROPE_BASE ** (-np.arange(half, dtype=np.float64) * 2.0 / head_width)
    def both(places):
        angles = places[:, None] * inverse[None, :]
        angles = np.concatenate([angles, angles], axis=1)
        return np.cos(angles).astype(np.float32), np.sin(angles).astype(np.float32)
    near = both(np.arange(rows, dtype=np.float64))
    far = both(np.arange(chunks, dtype=np.float64) * rows)
    return np.stack(near), np.stack(far, axis=1)


def layer_kernel(
    tokens, w_query, w_key, w_value, w_outer, w_inner, w_signal, near_in, wa_in, wc_in,
    gain_ref, far_ref, taps_ref, lam_ref, head_gain_ref,
    out_ref, lse_ref,
    tok, wqkv, wconv, wo, near, kv, q_all, q_stage, prod, gate, cv, cv_stage, att, att_stage,
    lse_in, lse_stage, lam_stage, lam_in, rs_in, rs_stage, rs_keep, acc, top, total,
    local_sem, tok_send, tok_recv, kv_to_p, kv_to_y, kv_to_z, kv_recv, q_send, q_recv,
    cv_send, cv_recv, edge_sem, att_send, att_recv, lse_send, lse_recv, wo_send, wo_recv,
    lam_sem, rs_send, rs_recv,
):
    s, t = lax.axis_index("sp"), lax.axis_index("tp")
    x, c = t // 2, t % 2
    y, zl, zh = s % 2, (s // 2) % 2, s // 4
    last = lax.axis_size("sp") - 1
    s1, s2, s4 = s + 1 - 2 * y, s + 2 - 4 * zl, s + 4 - 8 * zh
    s6 = s4 + 2 - 4 * zl
    t1, t2 = t + 1 - 2 * c, t + 2 - 4 * x
    owner = c == zl
    other = c != zl
    rows, width = tok.shape[1], tok.shape[2]
    block = tokens.shape[1]
    pieces = PIECES
    piece = rows // pieces
    pair = wqkv.shape[1] // 3
    hw = pair // 2
    halves = 2 * piece
    bf16, f32 = jnp.bfloat16, jnp.float32

    def remote(src, dst, ss, rs, dev):
        return pltpu.make_async_remote_copy(
            src_ref=src, dst_ref=dst, send_sem=ss, recv_sem=rs, device_id=dev, device_id_type=MESH
        )

    def span(p):
        return pl.ds(pl.multiple_of(p * piece, 16), piece)

    def cols(b):
        return pl.ds(pl.multiple_of(b * block, 128), block)

    own_cols = pl.ds(pl.multiple_of(zh * pair, 128), pair)
    loads = [
        pltpu.make_async_copy(tokens, tok.at[0, :, cols(t)], local_sem.at[0]),
        pltpu.make_async_copy(w_query.at[:, own_cols], wqkv.at[:, 0:pair], local_sem.at[1]),
        pltpu.make_async_copy(w_key.at[:, own_cols], wqkv.at[:, pair : 2 * pair], local_sem.at[2]),
        pltpu.make_async_copy(w_value.at[:, own_cols], wqkv.at[:, 2 * pair :], local_sem.at[3]),
        pltpu.make_async_copy(near_in, near, local_sem.at[4]),
        pltpu.make_async_copy(w_inner, wconv.at[0], local_sem.at[5]),
        pltpu.make_async_copy(w_signal, wconv.at[1], local_sem.at[6]),
        pltpu.make_async_copy(w_outer, wconv.at[2], local_sem.at[7]),
        pltpu.make_async_copy(wa_in, wo.at[c], local_sem.at[8]),
        pltpu.make_async_copy(wc_in, wo.at[2 + c], local_sem.at[9]),
    ]
    for load in loads:
        load.start()

    for hl in range(2):
        lam_stage[hl] = jnp.full(lam_stage.shape[1:], lam_ref[hl], f32)

    barrier = pltpu.get_barrier_semaphore()
    peers = [(s1, t), (s2, t), (s4, t), (s6, t), (s, t1), (s, t2), (s2, t1), (s4, t1), (s6, t1)]
    for peer in peers:
        pl.semaphore_signal(barrier, inc=1, device_id=peer, device_id_type=MESH)
    up_ok, down_ok = s < last, s > 0
    up, down = jnp.minimum(s + 1, last), jnp.maximum(s - 1, 0)

    @pl.when((y == 1) & up_ok)
    def _():
        pl.semaphore_signal(barrier, inc=1, device_id=(up, t), device_id_type=MESH)

    @pl.when((y == 0) & down_ok)
    def _():
        pl.semaphore_signal(barrier, inc=1, device_id=(down, t), device_id_type=MESH)

    across = jnp.where(y == 1, jnp.where(up_ok, 1, 0), jnp.where(down_ok, 1, 0))
    pl.semaphore_wait(barrier, len(peers) + across)

    def tok_at(k, p, b):
        return tok.at[k, span(p), cols(b)]

    def own_to_p(p):
        return remote(tokens.at[span(p)], tok_at(0, p, t), tok_send.at[0, p], tok_recv.at[0, 1, p], (s, t1))

    def own_to_x(p):
        return remote(tokens.at[span(p)], tok_at(0, p, t), tok_send.at[1, p], tok_recv.at[0, 2, p], (s, t2))

    def own_to_f(p):
        return remote(tokens.at[span(p)], tok_at(1, p, t), tok_send.at[2, p], tok_recv.at[1, 0, p], (s4, t))

    def mate_to_f(p):
        return remote(tok_at(0, p, t1), tok_at(1, p, t1), tok_send.at[3, p], tok_recv.at[1, 1, p], (s4, t))

    def cross_to_p(k, p):
        return remote(
            tok_at(k, p, t2), tok_at(k, p, t2), tok_send.at[4 + 4 * k, p], tok_recv.at[k, 3, p], (s, t1)
        )

    def far_to_p(p):
        return remote(tok_at(1, p, t), tok_at(1, p, t), tok_send.at[5, p], tok_recv.at[1, 1, p], (s, t1))

    def mate_back(p):
        return remote(tok_at(1, p, t1), tok_at(1, p, t1), tok_send.at[6, p], tok_recv.at[1, 0, p], (s, t1))

    def far_to_x(p):
        return remote(tok_at(1, p, t), tok_at(1, p, t), tok_send.at[7, p], tok_recv.at[1, 2, p], (s, t2))

    def tok_got(k, index, p):
        block_of = (t, t1, t2, t1 + t2 - t)[index]
        here = tok_at(k, p, block_of)
        remote(here, here, tok_send.at[0, p], tok_recv.at[k, index, p], (s, t1)).wait_recv()

    def each(n, body, start=0):
        def one(i, carry):
            body(i)
            return carry

        lax.fori_loop(start, n, one, 0)

    def first_sends(p):
        own_to_x(p).start()
        own_to_p(p).start()

    each(pieces, first_sends)
    lam_copy = remote(lam_stage, lam_in, lam_sem.at[0], lam_sem.at[1], (s, t1))
    lam_copy.start()

    def to_f(p):
        @pl.when(owner)
        def _():
            own_to_f(p).start()
            mate_to_f(p).start()

    def second_sends(p):
        tok_got(0, 1, p)

        @pl.when(p < 2)
        def _():
            to_f(p)

    each(pieces, second_sends)
    wo_copies = (
        remote(wa_in, wo.at[c], wo_send.at[0], wo_recv.at[0], (s, t1)),
        remote(wc_in, wo.at[2 + c], wo_send.at[1], wo_recv.at[1], (s, t1)),
    )
    for one_copy in wo_copies:
        one_copy.start()

    acc[...] = jnp.zeros_like(acc)
    total[...] = jnp.zeros_like(total)
    top[...] = jnp.full_like(top, MASKED)
    for load in loads:
        load.wait()

    def made(k):
        return jnp.where(owner, 4 * k, 8 + k)

    def kv_at(slot, p):
        return kv.at[slot, span(p)]

    def kv_p(slot, p):
        return remote(kv_at(slot, p), kv_at(slot, p), kv_to_p.at[slot, p], kv_recv.at[slot, p], (s, t1))

    def kv_y(slot, p):
        return remote(
            kv_at(slot, p), kv_at(slot + 1, p), kv_to_y.at[slot // 2, p], kv_recv.at[slot + 1, p], (s1, t)
        )

    def kv_z(k, p):
        return remote(
            kv_at(8 + k, p), kv_at(4 * k + 2, p), kv_to_z.at[k, p], kv_recv.at[4 * k + 2, p], (s2, t)
        )

    def q_rows(p):
        return pl.ds(pl.multiple_of((p // 2) * piece, 16), piece)

    def q_home(k, p):
        return remote(
            q_stage.at[k, span(p)], q_all.at[2 * k, q_rows(p)], q_send.at[k, p],
            q_recv.at[2 * k, p // 2], (s, t1),
        )

    def q_away(k, p):
        return remote(
            q_stage.at[k, span(p)], q_all.at[2 * k + 1, q_rows(p)], q_send.at[k, p],
            q_recv.at[2 * k + 1, p // 2], (s2, 2 * x + p % 2),
        )

    def ship(k, p):
        @pl.when(owner)
        def _():
            kv_y(4 * k, p).start()
            kv_p(4 * k, p).start()

            @pl.when(p % 2 != c)
            def _():
                q_home(k, p).start()

        @pl.when(other)
        def _():
            kv_z(k, p).start()
            q_away(k, p).start()

    def pass_on(slot, p):
        @pl.when(owner)
        def _():
            kv_p(slot, p).wait_recv()
            if slot % 2 == 0:
                kv_y(slot, p).start()
            kv_p(slot, p).start()

    def need(slot, low=0, high=PIECES):
        @pl.when(other)
        def _():
            each(high, lambda p: kv_p(slot, p).wait_recv(), start=low)

    sign = jnp.where(lax.broadcasted_iota(jnp.int32, (1, hw), 1) < hw // 2, -1.0, 1.0)

    def scaled_of(k, p):
        widened = tok[k, span(p), :].astype(f32)
        scaled = (widened * gain_ref[...]).astype(bf16)
        mean = jnp.sum(widened * widened, axis=1, keepdims=True) / width
        return scaled, lax.rsqrt(mean + NORM_EPS)

    def project_qkv(k, p, scaled, inv_rms):
        chunk = s if k == 0 else s4
        near_cos, near_sin = near[0, span(p), :], near[1, span(p), :]
        far_cos, far_sin = far_ref[chunk, 0:1, :], far_ref[chunk, 1:2, :]
        cosine = far_cos * near_cos - far_sin * near_sin
        sine = (far_sin * near_cos + far_cos * near_sin) * sign

        def rotary(v):
            return v * cosine + pltpu.roll(v, hw // 2, 1) * sine

        out = jnp.dot(scaled, wqkv[...], preferred_element_type=f32) * inv_rms
        slot = made(k)
        factor = hw ** (-0.5) * LOG2E
        queries = [(rotary(out[:, j * hw : (j + 1) * hw]) * factor).astype(bf16) for j in range(2)]
        for j in range(2):
            place = slice(pair + j * hw, pair + (j + 1) * hw)
            kv[slot, span(p), j * hw : (j + 1) * hw] = rotary(out[:, place]).astype(bf16)
        kv[slot, span(p), pair:] = out[:, 2 * pair :].astype(bf16)
        stay = owner & (p % 2 == c)

        @pl.when(stay)
        def _():
            for j in range(2):
                q_all[2 * k, q_rows(p), j * hw : (j + 1) * hw] = queries[j]

        @pl.when(jnp.logical_not(stay))
        def _():
            for j in range(2):
                q_stage[k, span(p), j * hw : (j + 1) * hw] = queries[j]

    def fill(p):
        scaled, inv_rms = scaled_of(0, p)
        inner = jnp.dot(scaled, wconv[0], preferred_element_type=f32) * inv_rms
        signal = jnp.dot(scaled, wconv[1], preferred_element_type=f32) * inv_rms
        prod[pl.ds(pl.multiple_of(8 + p * piece, 8), piece), :] = inner * signal
        gate[span(p), :] = jnp.dot(scaled, wconv[2], preferred_element_type=f32) * inv_rms

    def cross(k, p):
        tok_got(k, 2, p)
        cross_to_p(k, p).start()

    def finish_piece(k, p):
        tok_got(k, 3, p)
        scaled, inv_rms = scaled_of(k, p)
        project_qkv(k, p, scaled, inv_rms)
        ship(k, p)

    def own_piece(p):
        @pl.when(p == pieces - 1)
        def _():
            to_f(2)

        cross(0, p)
        finish_piece(0, p)

    each(pieces, own_piece)

    edge = remote(prod.at[rows : rows + 8], prod.at[0:8], edge_sem.at[0], edge_sem.at[1], (up, t))

    def far_forward(p):
        @pl.when(owner)
        def _():
            tok_got(1, 0, p)
            far_to_x(p).start()
            far_to_p(p).start()
            tok_got(1, 1, p)
            mate_back(p).start()

        @pl.when(other)
        def _():
            tok_got(1, 0, p)
            far_to_x(p).start()
            tok_got(1, 1, p)

    def pass_all(slot, low=0, high=PIECES):
        each(high, functools.partial(pass_on, slot), start=low)

    def xor(a, b):
        return a + b - 2 * a * b

    def level_of(k):
        return 2 * xor(zh, k // 2) + xor(zl, k % 2)

    lanes = top.shape[3]

    def absorb(jq, here, keys, values, seen=None):
        new_top, lifted, olds = [], [], []
        for m in range(2):
            place = slice(m * hw, (m + 1) * hw)
            scores = lax.dot_general(
                q_all[jq, here, place], keys(place), (((1,), (1,)), ((), ())),
                preferred_element_type=f32,
            )
            if seen is not None:
                scores = jnp.where(seen, scores, MASKED)
            lifted.append(scores)
            olds.append(top[jq, m, here, :])
        count = lifted[0].shape[1] // lanes
        parts = [[v[:, n * lanes : (n + 1) * lanes] for n in range(count)] for v in lifted]
        for m in range(2):
            best = functools.reduce(jnp.maximum, parts[m])
            new_top.append(jnp.maximum(olds[m], jnp.max(best, axis=1, keepdims=True)))
        raised = [[jnp.exp2(v - new_top[m]) for v in parts[m]] for m in range(2)]
        shrink = [jnp.exp2(olds[m] - new_top[m]) for m in range(2)]
        sums = [shrink[m] * total[jq, m, here, :] + functools.reduce(jnp.add, raised[m]) for m in range(2)]
        block_values = values()
        added = [
            jnp.dot(
                jnp.concatenate([v.astype(bf16) for v in raised[m]], axis=1), block_values,
                preferred_element_type=f32,
            )
            for m in range(2)
        ]
        wide = [jnp.concatenate([shrink[m]] * (pair // lanes), axis=1) for m in range(2)]
        grown = [wide[m] * acc[jq, m, here, :] + added[m] for m in range(2)]
        for m in range(2):
            top[jq, m, here, :] = new_top[m]
            total[jq, m, here, :] = sums[m]
            acc[jq, m, here, :] = grown[m]

    def part_of(i):
        return pl.ds(pl.multiple_of(i * piece, 16), piece)

    def both(jq, i, kp, low=0, high=None):
        high = rows if high is None else high

        def keys(place):
            return kv[pl.ds(2 * kp, 2), low:high, place].reshape(2 * (high - low), hw)

        def values():
            return kv[pl.ds(2 * kp, 2), low:high, pair:].reshape(2 * (high - low), pair)

        absorb(jq, part_of(i), keys, values)

    def beside(jq, i):
        slot = 2 * jq + 1
        absorb(jq, part_of(i), lambda place: kv[slot, :, place], lambda: kv[slot, :, pair:])

    def diagonal(jq, i):
        slot = 2 * jq
        for half in range(2):
            @pl.when(i == half)
            def _():
                length = (2 * half + 2) * piece
                query_at = (2 * half + c) * piece + lax.broadcasted_iota(jnp.int32, (piece, length), 0)
                key_at = lax.broadcasted_iota(jnp.int32, (piece, length), 1)
                absorb(
                    jq, part_of(i), lambda place: kv[slot, :length, place],
                    lambda: kv[slot, :length, pair:], key_at <= query_at,
                )

    def q_got(jq, i):
        def one():
            here = q_all.at[jq, q_rows(2 * i)]
            remote(here, here, q_send.at[0, 0], q_recv.at[jq, i], (s, t1)).wait_recv()

        if jq % 2 == 1:
            one()
        else:
            pl.when(other)(one)

    far_forward(0)
    to_f(3)
    far_forward(1)
    fill(0)
    pass_all(1)
    cross(1, 0)

    def far_piece(p):
        finish_piece(1, p)

        @pl.when((p > 0) & (p < pieces - 1))
        def _():
            far_forward(p + 1)

        @pl.when(p == 1)
        def _():
            pass_all(2)

        @pl.when(p == 3)
        def _():
            pass_on(6, 0)

        @pl.when(p < pieces - 1)
        def _():
            fill(p + 1)

            @pl.when(p == 1)
            def _():
                need(0)
                q_got(0, 0)
                q_got(0, 1)
                each(2, lambda i: diagonal(0, i))

            cross(1, p + 1)

    each(pieces, far_piece)

    @pl.when(up_ok)
    def _():
        edge.start()

    lam_copy.wait_recv()
    lam = jnp.where(owner, lam_stage[zh, 0:1, :], lam_in[zh, 0:1, :])
    lam = jnp.concatenate([lam] * (pair // lanes), axis=1)
    gain = head_gain_ref[...] * HEAD_KEEP
    home = 2 * zl + zh

    def seat(jq):
        return 2 * level_of(jq) + y

    def att_away(jq, i):
        return remote(
            att_stage.at[jq - 1, part_of(i)], att.at[home, part_of(i)], att_send.at[jq - 1, i],
            att_recv.at[jq - 1, i], (seat(jq), t),
        )

    def att_got(jq, i):
        here = att.at[0, part_of(i)]
        remote(here, here, att_send.at[jq - 1, i], att_recv.at[jq - 1, i], (seat(jq), t)).wait_recv()

    def lse_away(jq):
        return remote(
            lse_stage.at[jq], lse_in.at[zh, c], lse_send.at[jq], lse_recv.at[zh, c],
            (seat(jq), 2 * x + zl),
        )

    def close(jq, i, now):
        here = part_of(i)
        parts = [
            acc[jq, m, here, :] / jnp.sum(total[jq, m, here, :], axis=1, keepdims=True) for m in range(2)
        ]
        difference = parts[0] - lam * parts[1]
        mean = jnp.mean(difference * difference, axis=1, keepdims=True)
        result = (difference * lax.rsqrt(mean + NORM_EPS) * gain).astype(bf16)

        @pl.when(jq == 0)
        def _():
            att[home, here, :] = result

        @pl.when(jq > 0)
        def _():
            att_stage[jq - 1, here, :] = result

            @pl.when(now)
            def _():
                att_away(jq, i).start()

    half = pieces // 2
    pass_all(5, 0, 3)
    need(2)
    q_got(1, 0)
    q_got(1, 1)
    each(2, lambda i: diagonal(1, i))
    pass_on(6, 1)
    pass_all(3)

    def near_level(n):
        jq, i = n // 2, n % 2

        @pl.when(level_of(1 - jq) < level_of(jq))
        def _():
            both(jq, i, 1 - jq)

        @pl.when(y == 1)
        def _():
            beside(jq, i)

    need(1)
    need(3)
    each(4, near_level)

    @pl.when(zh == 0)
    def _():
        each(4, lambda n: close(1 - n // 2, n % 2, True))

    pass_on(6, 2)
    pass_on(5, 3)
    pass_all(7, 0, half)
    for slot in (4, 5, 6, 7):
        need(slot, 0, half)
    q_got(2, 0)
    q_got(3, 0)

    @pl.when(zh == 1)
    def _():
        each(8, lambda n: both(n // 4, (n // 2) % 2, 2 + n % 2, 0, halves))

    @pl.when(zh == 0)
    def _():
        each(4, lambda n: both(2 + n // 2, 0, n % 2))

    pass_on(6, 3)
    pass_on(7, 2)
    q_got(2, 1)
    q_got(3, 1)

    @pl.when(zh == 0)
    def _():
        each(4, lambda n: both(2 + n // 2, 1, n % 2))

    @pl.when(down_ok)
    def _():
        edge.wait_recv()

    @pl.when(jnp.logical_not(down_ok))
    def _():
        prod[0:8, :] = jnp.zeros((8, prod.shape[1]), f32)

    taps = taps_ref[...].astype(f32)
    for p in range(pieces):
        begin = 8 + p * piece
        smoothed = (
            taps[0:1] * prod[begin - 2 : begin - 2 + piece, :]
            + taps[1:2] * prod[begin - 1 : begin - 1 + piece, :]
            + taps[2:3] * prod[begin : begin + piece, :]
        )
        convolved = (gate[p * piece : (p + 1) * piece, :] * smoothed).astype(bf16)
        place = slice((p // 2) * piece, (p // 2 + 1) * piece)

        @pl.when(c == p % 2)
        def _():
            cv[c, place, :] = convolved

        @pl.when(c != p % 2)
        def _():
            cv_stage[place, :] = convolved

    cv_copy = remote(cv_stage, cv.at[c], cv_send.at[0], cv_recv.at[0], (s, t1))
    cv_copy.start()

    pass_on(7, 3)
    for slot in (4, 5, 6, 7):
        need(slot, half)

    def one_slot(i, n, now):
        jq = jnp.where(n < 2, n + 2, 3 - n)

        def one_level(kp):
            @pl.when((level_of(kp) < level_of(jq)) & (jq >= 2) & (kp >= 2))
            def _():
                both(jq, i, kp)

            @pl.when((level_of(kp) < level_of(jq)) & (jq < 2) & (kp >= 2))
            def _():
                both(jq, i, kp, halves, rows)

        each(4, one_level)

        @pl.when(jq >= 2)
        def _():
            @pl.when(y == 1)
            def _():
                beside(jq, i)

            diagonal(jq, i)

        @pl.when((jq >= 2) | (zh == 1))
        def _():
            close(jq, i, now)

    def one_job(n):
        @pl.when(n == 6)
        def _():
            cv_copy.wait_recv()
            for one_copy in wo_copies:
                one_copy.wait_recv()
            for jq in (1, 2, 3):
                att_got(jq, 1 - x)
            each(n_cols, give)
            for jq in (2, 3):
                att_away(jq, x).start()

        one_slot(jnp.where(n < 4, 1 - x, x), n % 4, (n < 4) | (n >= 6))

    n_cols = rs_in.shape[0]
    step = rs_in.shape[2]

    def partial(i, n):
        part = pl.ds(pl.multiple_of(i * piece, 16), piece)
        out_cols = pl.ds(pl.multiple_of(n * step, 128), step)
        result = None
        for h in range(4):
            term = jnp.dot(
                att[h, part, :], wo[h // 2, (h % 2) * pair : (h % 2 + 1) * pair, out_cols],
                preferred_element_type=f32,
            )
            result = term if result is None else result + term
        for core in range(2):
            result = result + jnp.dot(cv[core, part, :], wo[2 + core, :, out_cols], preferred_element_type=f32)
        return result

    def rs_copy(n):
        return remote(rs_stage.at[n], rs_in.at[n], rs_send.at[n], rs_recv.at[n], (s, t2))

    def give(n):
        rs_stage[n] = partial(1 - x, n).astype(bf16)
        rs_copy(n).start()

    each(8, one_job)
    for jq in (3, 2, 1, 0):
        tops = [
            top[jq, m] * (1.0 / LOG2E) + jnp.log(jnp.sum(total[jq, m], axis=1, keepdims=True))
            for m in range(2)
        ]
        lane = lax.broadcasted_iota(jnp.int32, tops[0].shape, 1)
        turned = jnp.where(lane == 0, tops[0], tops[1]).T[0:8, :]
        if jq == 0:
            @pl.when(owner)
            def _():
                lse_in[zh, c] = turned

            @pl.when(other)
            def _():
                lse_stage[jq] = turned
                lse_away(jq).start()
        else:
            lse_stage[jq] = turned
            lse_away(jq).start()

    for jq in (1, 2, 3):
        att_got(jq, x)

    def keep(n):
        rs_keep[n] = partial(x, n)

    each(n_cols, keep)

    def lse_got(hl, cc):
        here = lse_in.at[hl, cc]

        @pl.when(jnp.logical_not((zl == c) & (zh == hl) & (cc == c)))
        def _():
            remote(here, here, lse_send.at[0], lse_recv.at[hl, cc], (s, t1)).wait_recv()

    for hl in range(2):
        for cc in range(2):
            lse_got(hl, cc)
    for cc in range(2):
        both_heads = jnp.concatenate(
            [lse_in[0, cc, 0:2], lse_in[1, cc, 0:2], jnp.zeros((lanes - 4, halves), f32)], axis=0
        ).T
        for i in range(2):
            begin = (2 * i + cc) * piece
            lse_ref[begin : begin + piece, :] = both_heads[i * piece : (i + 1) * piece, 0:4]

    for n in range(n_cols):
        rs_copy(n).wait_recv()
        out_ref[:, n * step : (n + 1) * step] = (rs_keep[n] + rs_in[n].astype(f32)).astype(bf16)

    lam_copy.wait_send()
    for one_copy in wo_copies:
        one_copy.wait_send()
    cv_copy.wait_send()

    @pl.when(up_ok)
    def _():
        edge.wait_send()

    def drain(p):
        own_to_p(p).wait_send()
        own_to_x(p).wait_send()
        far_to_x(p).wait_send()
        for k in range(2):
            cross_to_p(k, p).wait_send()

        @pl.when(owner)
        def _():
            own_to_f(p).wait_send()
            mate_to_f(p).wait_send()
            far_to_p(p).wait_send()
            mate_back(p).wait_send()
            for slot in range(8):
                kv_p(slot, p).wait_send()
                if slot % 2 == 0:
                    kv_y(slot, p).wait_send()
            for k in range(2):
                @pl.when(p % 2 != c)
                def _():
                    q_home(k, p).wait_send()

        @pl.when(other)
        def _():
            for k in range(2):
                kv_z(k, p).wait_send()
                q_away(k, p).wait_send()

    each(pieces, drain)
    for jq in (1, 2, 3):
        for i in range(2):
            att_away(jq, i).wait_send()
        lse_away(jq).wait_send()

    @pl.when(other)
    def _():
        lse_away(0).wait_send()

    each(n_cols, lambda n: rs_copy(n).wait_send())


def whole_layer(
    tokens, norm_gain, w_query, w_key, w_value, w_outer, w_inner, w_signal, conv_taps, lambdas,
    head_gain, attend_proj, convolve_proj,
):
    rows, block = tokens.shape
    width = norm_gain.shape[0]
    chunks = lax.axis_size("sp")
    head_count = lambdas.shape[0]
    pair = w_query.shape[1] // head_count
    channels = w_inner.shape[1]
    piece = rows // PIECES
    near, far = table_of(rows, chunks, pair // 2)
    n_cols = 4
    step = width // n_cols
    vmem = pl.BlockSpec(memory_space=pltpu.VMEM)
    anywhere = pl.BlockSpec(memory_space=pl.ANY)
    bf16, f32 = jnp.bfloat16, jnp.float32
    dma = pltpu.SemaphoreType.DMA
    mixed, lse = pl.pallas_call(
        layer_kernel,
        out_shape=(
            jax.ShapeDtypeStruct((piece, width), bf16),
            jax.ShapeDtypeStruct((rows, 2 * head_count), f32),
        ),
        in_specs=[anywhere] * 10 + [vmem] * 3 + [pl.BlockSpec(memory_space=pltpu.SMEM), vmem],
        out_specs=(vmem, vmem),
        scratch_shapes=[
            pltpu.VMEM((2, rows, width), bf16),
            pltpu.VMEM((width, 3 * pair), bf16),
            pltpu.VMEM((3, width, channels), bf16),
            pltpu.VMEM((4, channels, width), bf16),
            pltpu.VMEM(near.shape, f32),
            pltpu.VMEM((10, rows, 2 * pair), bf16),
            pltpu.VMEM((4, 2 * piece, pair), bf16),
            pltpu.VMEM((2, rows, pair), bf16),
            pltpu.VMEM((rows + 8, channels), f32),
            pltpu.VMEM((rows, channels), f32),
            pltpu.VMEM((2, 2 * piece, channels), bf16),
            pltpu.VMEM((2 * piece, channels), bf16),
            pltpu.VMEM((4, 2 * piece, pair), bf16),
            pltpu.VMEM((3, 2 * piece, pair), bf16),
            pltpu.VMEM((2, 2, 8, 2 * piece), f32),
            pltpu.VMEM((4, 8, 2 * piece), f32),
            pltpu.VMEM((head_count, 8, 128), f32),
            pltpu.VMEM((head_count, 8, 128), f32),
            pltpu.VMEM((n_cols, piece, step), bf16),
            pltpu.VMEM((n_cols, piece, step), bf16),
            pltpu.VMEM((n_cols, piece, step), f32),
            pltpu.VMEM((4, 2, 2 * piece, pair), f32),
            pltpu.VMEM((4, 2, 2 * piece, 128), f32),
            pltpu.VMEM((4, 2, 2 * piece, 128), f32),
            dma((10,)),
            dma((9, PIECES)),
            dma((2, 4, PIECES)),
            dma((8, PIECES)),
            dma((4, PIECES)),
            dma((2, PIECES)),
            dma((8, PIECES)),
            dma((2, PIECES)),
            dma((4, 2)),
            dma((1,)),
            dma((1,)),
            dma((2,)),
            dma((3, 2)),
            dma((3, 2)),
            dma((4,)),
            dma((2, 2)),
            dma((2,)),
            dma((2,)),
            dma((2,)),
            dma((n_cols,)),
            dma((n_cols,)),
        ],
        compiler_params=pltpu.CompilerParams(
            collective_id=0, has_side_effects=True, vmem_limit_bytes=63 * 2**20
        ),
        name="whole_layer",
    )(
        tokens, w_query, w_key, w_value, w_outer, w_inner, w_signal, jnp.asarray(near), attend_proj,
        convolve_proj, norm_gain[None, :], jnp.asarray(far), conv_taps, lambdas, head_gain[None, :],
    )
    return mixed, lse


def make_fold(groups, row_count, carry, pieces):
    key_piece, value_piece = pieces
    block_rows = min(key_piece.shape[0], row_count)
    shard_count = key_piece.shape[0] // block_rows

    def one_shard(inner_states, shard_index):
        first_key = shard_index * block_rows
        key_block = lax.dynamic_slice_in_dim(key_piece, shard_index * block_rows, block_rows, 0)
        value_block = lax.dynamic_slice_in_dim(value_piece, shard_index * block_rows, block_rows, 0)
        updated_states = []
        for given_state, group in zip(inner_states, groups):
            group_queries, group_places, group_last = group

            def take_block(given):
                return absorb(given, group_queries, group_places, key_block, value_block, first_key)

            def leave_block(given):
                return given

            updated_states.append(
                lax.cond(first_key < group_last, take_block, leave_block, given_state)
            )
        return (tuple(updated_states), None)

    carry, _ = lax.scan(one_shard, carry, jnp.arange(shard_count, dtype=jnp.int32))
    return carry


def attention_by_rows(query_sums, key_sums, value_sums, lambdas, head_gain, positions):
    row_count = query_sums.shape[0]
    head_count = lambdas.shape[0]
    head_width = query_sums.shape[1] // (2 * head_count)
    offset = lax.axis_index("sp") * row_count
    split = (row_count, 2 * head_count, head_width)
    queries = rotate(query_sums.reshape(split), positions).astype(jnp.bfloat16)
    key_rows = rotate(key_sums.reshape(split), positions).astype(jnp.bfloat16)
    value_rows = value_sums.astype(jnp.bfloat16)
    half_rows = row_count // 2
    bit_count = lax.axis_size("sp").bit_length() - 1
    handed = queries[half_rows:]
    for bit_index in range(bit_count):
        handed = partner(handed, "sp", bit_index)
    mirror = lax.axis_size("sp") - 1 - lax.axis_index("sp")
    mirror_start = mirror * row_count + half_rows
    mirror_places = mirror_start + jnp.arange(half_rows, dtype=jnp.int32)
    groups = (
        (queries[:half_rows], positions[:half_rows], offset + half_rows),
        (handed, mirror_places, mirror_start + half_rows),
    )
    initial = (
        empty_state(head_count, half_rows, head_width),
        empty_state(head_count, half_rows, head_width),
    )
    states = make_fold(
        groups,
        row_count,
        initial,
        (
            lax.all_gather(key_rows, "sp", axis=0, tiled=True),
            lax.all_gather(value_rows, "sp", axis=0, tiled=True),
        ),
    )
    own_attended, own_lse = finish(states[0], lambdas, head_gain)
    answer = finish(states[1], lambdas, head_gain)
    for bit_index in range(bit_count):
        answer = (
            partner(answer[0], "sp", bit_index),
            partner(answer[1].astype(jnp.bfloat16), "sp", bit_index).astype(jnp.float32),
        )
    attended = jnp.concatenate([own_attended, answer[0]], axis=0)
    row_lse = jnp.concatenate([own_lse, answer[1]], axis=0)
    return (attended, row_lse)


def per_device(
    tokens,
    norm_gain,
    w_query,
    w_key,
    w_value,
    w_outer,
    w_inner,
    w_signal,
    conv_taps,
    lambdas,
    head_gain,
    attend_proj,
    convolve_proj,
):
    row_count = tokens.shape[0]
    model_width = norm_gain.shape[0]
    head_count = lambdas.shape[0]
    head_width = w_query.shape[1] // (2 * head_count)
    count = lax.axis_size("sp")
    fits = count == 8 and lax.axis_size("tp") == 4 and head_count == 2 and head_width == 128
    if fits and row_count % (16 * PIECES) == 0 and w_inner.shape[1] == w_query.shape[1]:
        return whole_layer(
            tokens, norm_gain, w_query, w_key, w_value, w_outer, w_inner, w_signal, conv_taps,
            lambdas, head_gain, attend_proj, convolve_proj,
        )
    gathered = lax.all_gather(tokens, "tp", axis=1, tiled=True)
    widened = gathered.astype(jnp.float32)
    scaled = (widened * norm_gain[None, :]).astype(jnp.bfloat16)
    squares = jnp.sum(widened * widened, axis=1)
    inv_rms = lax.rsqrt(squares / model_width + NORM_EPS)[:, None]
    offset = lax.axis_index("sp") * row_count
    positions = offset + jnp.arange(row_count, dtype=jnp.int32)

    def product_of(weight):
        return inv_rms * jnp.dot(scaled, weight, preferred_element_type=jnp.float32)

    if head_count == 2 and head_width == 128 and count % 2 == 0:
        attended, row_lse = attention_by_head(
            gathered, norm_gain, w_query, w_key, w_value, lambdas, head_gain, positions
        )
    else:
        attended, row_lse = attention_by_rows(
            product_of(w_query),
            product_of(w_key),
            product_of(w_value),
            lambdas,
            head_gain,
            positions,
        )
    outer_gate = product_of(w_outer)
    product = product_of(w_inner) * product_of(w_signal)
    border = passed_along(product[row_count - 2 :], "sp", 1)
    padded = jnp.concatenate([border, product], axis=0)
    tap_values = conv_taps.astype(jnp.float32)
    smoothed = (
        tap_values[0] * padded[:-2] + tap_values[1] * padded[1:-1] + tap_values[2] * padded[2:]
    )
    convolved = (outer_gate * smoothed).astype(jnp.bfloat16)
    mixed = lax.psum_scatter(
        (
            jnp.dot(attended, attend_proj, preferred_element_type=jnp.float32)
            + jnp.dot(convolved, convolve_proj, preferred_element_type=jnp.float32)
        ).astype(jnp.bfloat16),
        "tp",
        scatter_dimension=0,
        tiled=True,
    )
    return (mixed, row_lse)


def solution(mesh):
    return jax.shard_map(
        per_device,
        mesh=mesh,
        in_specs=(
            P("sp", "tp"),
            P(),
            P(None, "tp"),
            P(None, "tp"),
            P(None, "tp"),
            P(None, "tp"),
            P(None, "tp"),
            P(None, "tp"),
            P(None, "tp"),
            P("tp"),
            P(),
            P("tp", None),
            P("tp", None),
        ),
        out_specs=(P(("sp", "tp"), None), P("sp", "tp")),
        check_vma=False,
    )
```
